128 devices in a mesh: ep: 32 (over z, y, core), tp: 4 (over x).
Axes of the slice: x: 4, y: 4, z: 4, core: 2. Of those that a mesh axis runs over, the one named last changes fastest.
Arguments:
- tokens: bfloat16 [1536, 2048], P(('ep', 'tp')), may hold values from -6 to 6
- cache_latent: bfloat16 [1536, 1024, 512], P(('ep', 'tp')), may hold values from -1700 to 1700
- cache_rope: bfloat16 [1536, 64, 1024], P(('ep', 'tp')), may hold values from -6 to 6
- lengths: int32 [1536], P(('ep', 'tp')), may hold values from 128 to 1023, as said below
- attn_gain: bfloat16 [2048], replicated, may hold values from 0.099609375 to 1.8984375
- latent_gain: bfloat16 [512], replicated, may hold values from 0.099609375 to 1.8984375
- post_attn_gain: bfloat16 [2048], replicated, may hold values from 0.099609375 to 1.8984375
- ffn_gain: bfloat16 [2048], replicated, may hold values from 0.099609375 to 1.8984375
- post_ffn_gain: bfloat16 [2048], replicated, may hold values from 0.099609375 to 1.8984375
- w_query: bfloat16 [2048, 2048], P(None, 'tp'), may hold values from -0.125 to 0.125
- w_query_rot: bfloat16 [2048, 1024], P(None, 'tp'), may hold values from -0.125 to 0.125
- w_latent: bfloat16 [2048, 512], P(None, 'tp'), may hold values from -0.125 to 0.125
- w_key_rot: bfloat16 [2048, 64], replicated, may hold values from -0.125 to 0.125
- w_key_up: bfloat16 [512, 16, 128], P(None, 'tp'), may hold values from -0.25 to 0.25
- w_value_up: bfloat16 [512, 16, 128], P(None, 'tp'), may hold values from -0.25 to 0.25
- w_out: bfloat16 [2048, 2048], P('tp'), may hold values from -0.125 to 0.125
- route_logits: float32 [1536, 4], P('ep'), may hold values from -6 to 6
- routes: int32 [1536, 4], P('ep'), may hold values from 0 to 31, all different within a row; in each aligned block of 48 rows (0 to 47, 48 to 95, ...) at most 7 rows name the same one
- w_gate: bfloat16 [32, 2048, 2048], P('ep', None, 'tp'), may hold values from -0.3125 to 0.3125
- w_up: bfloat16 [32, 2048, 2048], P('ep', None, 'tp'), may hold values from -0.3125 to 0.3125
- w_down: bfloat16 [32, 2048, 2048], P('ep', 'tp'), may hold values from -0.125 to 0.125
Outputs:
- result: bfloat16 [1536, 2048], P(('ep', 'tp'))
- new_latent: bfloat16 [1536, 512], P(('ep', 'tp'))
- new_rope: bfloat16 [1536, 64], P(('ep', 'tp'))
The draws below stay inside these ranges and needn't reach their ends.
Inputs may be any that keep to these rules, and one draw needn't show every extreme that they name: Each sequence's cache holds positions 0 to lengths - 1, and the new token stands at position lengths; some sequence has 1023 in every draw. `routes`: each row names 4 different experts; in each aligned block of 48 rows (the tokens of one index of ep) no expert is named more than 7 times, a bound that some block reaches.
All inputs are finite; a program needn't handle non-finite values.
Results may differ from the reference program's by a relative error of at most 0.019.
Values may be sent and summed in bfloat16 or wider, within the bound.
A program may use at most 128 MiB of HBM per device.

```python
import math
import jax
import jax.numpy as jnp
import numpy as np
from jax import lax

D = 2048
HEADS = 16
KEY_DIM = 128
ROT_DIM = 64
VAL_DIM = 128
LATENT = 512
FF = 2048
TOP_K = 4
SEQ_DEV = 12
LEN = 1024
EXPERTS = 32
GROUP = 48
BATCH = 1536
CAP = 7
N_TP = 4


def draw_cache_latent(key, part):
    base_key = jax.random.fold_in(jax.random.fold_in(key, 11), 0)
    cache = jnp.clip(jax.random.normal(base_key, (BATCH, LEN, LATENT), jnp.float32), -5.0, 5.0)
    return cache.astype(jnp.bfloat16)


def draw_lengths(key, part):
    keys = jax.random.split(jax.random.fold_in(key, 23), 3)
    lowest = LEN // 8
    ceilings = jax.random.randint(keys[0], (BATCH // SEQ_DEV,), LEN // 4, LEN)
    ceilings = jnp.repeat(ceilings, SEQ_DEV)
    drawn = jax.random.randint(keys[1], (BATCH,), lowest, ceilings)
    longest = jax.random.randint(keys[2], (), 0, BATCH)
    return jnp.where(jnp.arange(BATCH) == longest, LEN - 1, drawn).astype(jnp.int32)


def block_levels(rng, shape, cuts, least, top_value):
    def one(position, shards_of):
        heights = jax.random.uniform(jax.random.fold_in(jax.random.fold_in(rng, 6), position), (shards_of,), jnp.float32, least / len(cuts), top_value / len(cuts))
        return jnp.repeat(jnp.exp(heights), shape[position] // shards_of).reshape((-1,) + (1,) * (len(shape) - position - 1))

    loudness = one(*cuts[0])
    for cut in cuts[1:]:
        loudness = loudness * one(*cut)
    return loudness


def assign_block(stream_key, own, number, rows, count, top, limit, lean):
    order = jax.random.permutation(stream_key, count)
    heavy_load, ordinary = shares(count, rows * top, limit, lean, True), shares(count, rows * top, limit, lean, False)
    places = jnp.arange(count)

    def named(sizes, offset_by):
        used = int((sizes > 0).sum())
        fixed = max(1, used // 4)
        shifted = fixed + (places - fixed + offset_by * (used - fixed)) % max(1, count - fixed)
        return jnp.zeros((count,), jnp.int32).at[order[jnp.where(places < fixed, places, shifted)]].set(jnp.asarray(sizes, jnp.int32))

    sizes = jnp.where(number % 4 == 0, named(heavy_load, number // 4), named(ordinary, number - number // 4 - 1))
    mixed = jax.random.permutation(jax.random.fold_in(own, 3), count)
    source_of, sink = mixed[0:count // 2 * 2:2], mixed[1:count // 2 * 2:2]
    room = jnp.minimum(sizes[source_of] - 1, limit - sizes[sink]) // 2
    room = jnp.where((source_of == order[0]) | (sink == order[0]) | (sizes[sink] == 0), 0, jnp.maximum(room, 0))
    shifted = jax.random.randint(jax.random.fold_in(own, 4), (count // 2,), 0, 1 << 20) % (room + 1)
    sizes = sizes.at[source_of].add(-shifted).at[sink].add(shifted)
    members = jnp.searchsorted(jnp.cumsum(sizes), jnp.arange(rows * top), side="right").astype(jnp.int32)
    table = members.reshape(top, rows).T
    table = table[jax.random.permutation(jax.random.fold_in(own, 1), rows)]
    offset_by = jax.random.randint(jax.random.fold_in(own, 2), (rows, 1), 0, top)
    return jnp.take_along_axis(table, (jnp.arange(top)[None, :] + offset_by) % top, axis=1)


def shares(number_of, total, bound, slope, full):
    loads = [(1 << 20) // math.isqrt(grade ** slope) + 1 for grade in range(1, number_of + 1)]
    largest = bound if full else min(bound, max(-(-total // number_of), total * loads[0] // sum(loads)))
    least = 1 if total - largest >= number_of - 1 else 0
    given, rest = [largest] + [least] * (number_of - 1), total - largest - least * (number_of - 1)
    while rest > 0:
        free = [i for i in range(1, number_of) if given[i] < largest] or [i for i in range(1, number_of) if given[i] < bound]
        pool, budget = sum([loads[i] for i in free]), rest
        for i in free:
            addition = min(bound - given[i], max(1, budget * loads[i] // pool), rest)
            given[i] = given[i] + addition
            rest = rest - addition
    return np.array(given)


def bell_draw(key, shape, scale, most, cuts=(), kind=jnp.bfloat16):
    values = scale * jax.random.normal(key, shape, jnp.float32)
    if cuts:
        values = values * block_levels(key, shape, cuts, -0.22, 0.18)
    return jnp.clip(values, -most, most).astype(kind)


def setup_inputs(seed: int = 0) -> dict:
    key_list = jax.random.split(jax.random.key(seed), 22)
    tokens = bell_draw(key_list[0], (BATCH, D), 1.0, 6.0, ((0, 128),))
    cache_latent = draw_cache_latent(jax.random.fold_in(key_list[21], 71), 0)
    cache_rope = bell_draw(key_list[2], (BATCH, ROT_DIM, LEN), 1.0, 6.0, ((0, 128),))
    lengths = draw_lengths(jax.random.fold_in(key_list[21], 71), 0)
    attn_gain = jnp.clip(1.0 + 0.18 * jax.random.normal(key_list[4], (D,), jnp.float32), 0.099609375, 1.8984375).astype(jnp.bfloat16)
    latent_gain = jnp.clip(1.0 + 0.18 * jax.random.normal(key_list[5], (LATENT,), jnp.float32), 0.099609375, 1.8984375).astype(jnp.bfloat16)
    post_attn_gain = jnp.clip(1.0 + 0.18 * jax.random.normal(key_list[6], (D,), jnp.float32), 0.099609375, 1.8984375).astype(jnp.bfloat16)
    ffn_gain = jnp.clip(1.0 + 0.18 * jax.random.normal(key_list[7], (D,), jnp.float32), 0.099609375, 1.8984375).astype(jnp.bfloat16)
    post_ffn_gain = jnp.clip(1.0 + 0.18 * jax.random.normal(key_list[8], (D,), jnp.float32), 0.099609375, 1.8984375).astype(jnp.bfloat16)
    w_query = bell_draw(key_list[9], (D, HEADS * KEY_DIM), D ** -0.5, 0.125, ((1, 4),))
    w_query_rot = bell_draw(key_list[10], (D, HEADS * ROT_DIM), D ** -0.5, 0.125, ((1, 4),))
    w_latent = bell_draw(key_list[11], (D, LATENT), D ** -0.5, 0.125, ((1, 4),))
    w_key_rot = bell_draw(key_list[12], (D, ROT_DIM), D ** -0.5, 0.125)
    w_key_up = bell_draw(key_list[13], (LATENT, HEADS, KEY_DIM), LATENT ** -0.5, 0.25, ((1, 4),))
    w_value_up = bell_draw(key_list[14], (LATENT, HEADS, VAL_DIM), LATENT ** -0.5, 0.25, ((1, 4),))
    w_out = bell_draw(key_list[15], (HEADS * VAL_DIM, D), (HEADS * VAL_DIM) ** -0.5, 0.125, ((0, 4),))
    route_logits = bell_draw(key_list[16], (BATCH, TOP_K), 1.0, 6.0, ((0, 32),), jnp.float32)
    routes_keys = jax.random.split(jax.random.fold_in(key_list[17], 1), BATCH // GROUP)
    routes_turns = jax.random.permutation(jax.random.fold_in(key_list[17], 3), BATCH // GROUP)
    routes = jax.vmap(lambda own, number: assign_block(jax.random.fold_in(key_list[17], 2), own, number, GROUP, EXPERTS, TOP_K, CAP, 2))(routes_keys, routes_turns).reshape((BATCH, TOP_K))
    w_gate = bell_draw(key_list[18], (EXPERTS, D, FF), 0.055, 0.3125, ((0, 32), (2, 4)))
    w_up = bell_draw(key_list[19], (EXPERTS, D, FF), 0.055, 0.3125, ((0, 32), (2, 4)))
    w_down = bell_draw(key_list[20], (EXPERTS, FF, D), FF ** -0.5, 0.125, ((0, 32), (1, 4)))
    return dict(tokens=tokens, cache_latent=cache_latent, cache_rope=cache_rope, lengths=lengths, attn_gain=attn_gain, latent_gain=latent_gain, post_attn_gain=post_attn_gain, ffn_gain=ffn_gain, post_ffn_gain=post_ffn_gain, w_query=w_query, w_query_rot=w_query_rot, w_latent=w_latent, w_key_rot=w_key_rot, w_key_up=w_key_up, w_value_up=w_value_up, w_out=w_out, route_logits=route_logits, routes=routes, w_gate=w_gate, w_up=w_up, w_down=w_down)


eps_norm = 1e-06
clamp_limit = 7.0
sigmoid_alpha = 1.702
theta_base = 10000.0

def rms_scale(values, gain):
    mean_square = lax.optimization_barrier(jnp.mean(values * values, axis=-1, keepdims=True))
    return values * lax.rsqrt(mean_square + eps_norm) * gain.astype(jnp.float32)

def rotate(values, positions):
    half = values.shape[-1] // 2
    freqs = theta_base ** (-jnp.arange(half, dtype=jnp.float32) / half)
    angles = positions[..., None] * freqs
    cosine = jnp.cos(angles)
    sine = jnp.sin(angles)
    first = values[..., :half]
    second = values[..., half:]
    return jnp.concatenate([first * cosine - second * sine, second * cosine + first * sine], axis=-1)

def reference(tokens, cache_latent, cache_rope, lengths, attn_gain, latent_gain, post_attn_gain, ffn_gain, post_ffn_gain, w_query, w_query_rot, w_latent, w_key_rot, w_key_up, w_value_up, w_out, route_logits, routes, w_gate, w_up, w_down):
    batch, width = tokens.shape
    latent_size, heads, key_size = w_key_up.shape
    rot_size = w_key_rot.shape[1]
    value_size = w_value_up.shape[2]
    span = cache_latent.shape[1]
    scale = (key_size + rot_size) ** (-0.5)
    token_values = tokens.astype(jnp.float32)
    normed = rms_scale(token_values, attn_gain).astype(jnp.bfloat16)
    query_plain = jnp.dot(normed, w_query, preferred_element_type=jnp.float32).astype(jnp.bfloat16)
    query_plain = query_plain.reshape(batch, heads, key_size)
    query_rotary = jnp.dot(normed, w_query_rot, preferred_element_type=jnp.float32).astype(jnp.bfloat16)
    query_rotary = query_rotary.reshape(batch, heads, rot_size)
    latent_raw = jnp.dot(normed, w_latent, preferred_element_type=jnp.float32).astype(jnp.bfloat16)
    key_raw = jnp.dot(normed, w_key_rot, preferred_element_type=jnp.float32).astype(jnp.bfloat16)
    new_latent = rms_scale(latent_raw.astype(jnp.float32), latent_gain).astype(jnp.bfloat16)
    positions = lengths.astype(jnp.float32)
    new_rope = rotate(key_raw.astype(jnp.float32), positions).astype(jnp.bfloat16)
    query_turned = rotate(query_rotary.astype(jnp.float32), positions[:, None]).astype(jnp.bfloat16)
    query_latent = jnp.einsum('bhn,chn->bhc', query_plain.astype(jnp.float32), w_key_up.astype(jnp.float32)).astype(jnp.bfloat16)

    def attend(pieces):
        q_lat, q_turn, latents, rotary, fresh_latent, fresh_rope, length = pieces
        latents_f = latents.astype(jnp.float32)
        scores = jnp.einsum('hc,pc->hp', q_lat.astype(jnp.float32), latents_f)
        scores = (scores + jnp.einsum('hr,rp->hp', q_turn.astype(jnp.float32), rotary.astype(jnp.float32))) * scale
        self_score = (lax.optimization_barrier(jnp.sum(q_lat.astype(jnp.float32) * fresh_latent.astype(jnp.float32)[None, :], axis=-1)) + lax.optimization_barrier(jnp.sum(q_turn.astype(jnp.float32) * fresh_rope.astype(jnp.float32)[None, :], axis=-1))) * scale
        valid = jnp.arange(span, dtype=jnp.int32) < length
        masked = jnp.where(valid[None, :], scores, -jnp.inf)
        highest = jnp.maximum(lax.optimization_barrier(jnp.max(masked, axis=-1)), self_score)
        raised = jnp.exp(masked - highest[:, None])
        raised_self = jnp.exp(self_score - highest)
        total = lax.optimization_barrier(jnp.sum(raised, axis=-1)) + raised_self
        probs = (raised / total[:, None]).astype(jnp.bfloat16)
        prob_self = (raised_self / total).astype(jnp.bfloat16)
        summed = jnp.einsum('hp,pc->hc', probs.astype(jnp.float32), latents_f)
        summed = summed + prob_self.astype(jnp.float32)[:, None] * fresh_latent.astype(jnp.float32)[None, :]
        return summed.astype(jnp.bfloat16)
    head_latent = lax.map(attend, (query_latent, query_turned, cache_latent, cache_rope, new_latent, new_rope, lengths))
    values = jnp.einsum('bhc,chv->bhv', head_latent.astype(jnp.float32), w_value_up.astype(jnp.float32)).astype(jnp.bfloat16)
    flat_values = values.reshape(batch, heads * value_size)
    group_cols = heads // N_TP * value_size
    attn = jnp.zeros((batch, width), jnp.float32)
    for section in range(N_TP):
        lower = section * group_cols
        partial_sum = jnp.dot(flat_values[:, lower:lower + group_cols], w_out[lower:lower + group_cols], preferred_element_type=jnp.float32).astype(jnp.bfloat16)
        attn = attn + partial_sum.astype(jnp.float32)
    attn = attn.astype(jnp.bfloat16)
    mixed = (token_values + rms_scale(attn.astype(jnp.float32), post_attn_gain)).astype(jnp.bfloat16)
    ffn_input = rms_scale(mixed.astype(jnp.float32), ffn_gain).astype(jnp.bfloat16)
    route_weights = jax.nn.softmax(route_logits, axis=-1)
    top_k = routes.shape[1]
    experts = w_gate.shape[0]
    hidden = w_gate.shape[2]
    n_blocks = batch // GROUP
    assigned = GROUP * top_k
    flat_routes = routes.reshape(n_blocks, assigned).astype(jnp.int32)
    onehot = (flat_routes[:, :, None] == jnp.arange(experts, dtype=jnp.int32)[None, None, :]).astype(jnp.int32)
    rank = lax.optimization_barrier(jnp.sum((jnp.cumsum(onehot, axis=1) - onehot) * onehot, axis=-1)).astype(jnp.int32)
    block_ids = jnp.broadcast_to(jnp.arange(n_blocks, dtype=jnp.int32)[:, None], (n_blocks, assigned))
    token_ids = (jnp.arange(assigned, dtype=jnp.int32) // top_k).astype(jnp.int32)
    rows_in = ffn_input.reshape(n_blocks, GROUP, width)
    gathered = rows_in[:, token_ids]
    slots = jnp.zeros((n_blocks, experts, CAP, width), jnp.bfloat16).at[block_ids, flat_routes, rank].set(gathered)
    block_hidden = hidden // N_TP

    def expert(pieces):
        rows, gate_weight, up_weight, down_weight = pieces
        flat = rows.reshape(-1, width)
        gate = jnp.minimum(jnp.dot(flat, gate_weight, preferred_element_type=jnp.float32), clamp_limit)
        upward = jnp.clip(jnp.dot(flat, up_weight, preferred_element_type=jnp.float32), -clamp_limit, clamp_limit)
        active = ((upward + 1.0) * gate * jax.nn.sigmoid(sigmoid_alpha * gate)).astype(jnp.bfloat16)
        total = jnp.zeros((flat.shape[0], width), jnp.float32)
        for section in range(N_TP):
            lower = section * block_hidden
            piece = jnp.dot(active[:, lower:lower + block_hidden], down_weight[lower:lower + block_hidden], preferred_element_type=jnp.float32).astype(jnp.bfloat16)
            total = total + piece.astype(jnp.float32)
        return total.astype(jnp.bfloat16).reshape(rows.shape)
    outputs = lax.map(expert, (jnp.moveaxis(slots, 1, 0), w_gate, w_up, w_down))
    picked = outputs[flat_routes, block_ids, rank].astype(jnp.float32).reshape(batch, top_k, width)
    moe = lax.optimization_barrier(jnp.sum(picked * route_weights[:, :, None], axis=1)).astype(jnp.bfloat16)
    result = (mixed.astype(jnp.float32) + rms_scale(moe.astype(jnp.float32), post_ffn_gain)).astype(jnp.bfloat16)
    return (result, new_latent, new_rope)
```

```python
import functools
import math

import jax
import jax.numpy as jnp
from jax import lax
from jax.experimental import pallas as pl
from jax.experimental.pallas import tpu as pltpu
from jax.sharding import PartitionSpec as P

MESH = pl.DeviceIdType.MESH
eps_norm = 1e-06
clamp_limit = 7.0
sigmoid_alpha = 1.702
theta_base = 10000.0
f32 = jnp.float32
bf16 = jnp.bfloat16

SEQ = 12
PAD = 16
D = 2048
LAT = 512
ROT = 64
LEN = 1024
HL = 4
TP = 4
EP = 32
CAPP = 8
MSG = HL * LAT + HL * ROT + 128


def hops(a):
    return min(a, 4 - a)


far_first = sorted(range(1, EP), key=lambda d: -(hops(d // 8) + hops((d // 2) % 4)))


def ep_shift(me, d, sign):
    z, y, c = me // 8, (me // 2) % 4, me % 2
    dz, dy, dc = d // 8, (d // 2) % 4, d % 2
    if sign < 0:
        dz, dy = (4 - dz) % 4, (4 - dy) % 4
    return ((z + dz) % 4) * 8 + ((y + dy) % 4) * 2 + (c + dc) % 2


def mm(a, b):
    return lax.dot_general(a, b, (((1,), (0,)), ((), ())), preferred_element_type=f32)


def mm_nt(a, b):
    return lax.dot_general(a, b, (((1,), (1,)), ((), ())), preferred_element_type=f32)


def rms(v, gain):
    mean_square = jnp.mean(v * v, axis=-1, keepdims=True)
    return v * lax.rsqrt(mean_square + eps_norm) * gain


def layer_kernel(
    lens,
    tok_in,
    routes_in,
    logits_in,
    g_attn,
    g_lat,
    g_post,
    g_ffn,
    g_post2,
    h_clat,
    h_crope,
    h_wq,
    h_wqr,
    h_wl,
    h_wkr,
    h_wku,
    h_wvu,
    h_wo,
    h_wg,
    h_wu,
    h_wd,
    out_ref,
    lat_ref,
    rope_ref,
    tok32,
    nbuf,
    wq,
    wqr,
    wl,
    wkr,
    wku,
    wvu,
    wtmp,
    wkh,
    wvh,
    msg_s,
    msg_r,
    cache,
    rope,
    A,
    A2,
    Q,
    Qr,
    S,
    Pb,
    ps_ref,
    O,
    hl_s,
    hl_r,
    wo,
    p_s,
    p_r,
    gbuf,
    mixed_ref,
    r64,
    l64,
    Dm,
    Cm,
    X,
    R,
    Y,
    T,
    wg,
    wu,
    wd,
    m_s,
    m_r,
    lsem,
    csem,
    rsem,
    tss,
    trs,
    dss,
    drs,
    ess,
    ers,
):
    me = lax.axis_index("ep")
    t = lax.axis_index("tp")
    barrier = pltpu.get_barrier_semaphore()
    for d in (1, 2, 3):
        pl.semaphore_signal(barrier, inc=1, device_id={"tp": (t + d) % TP}, device_id_type=MESH)
    for d in far_first:
        pl.semaphore_signal(barrier, inc=1, device_id={"ep": ep_shift(me, d, 1)}, device_id_type=MESH)

    def local(src, dst, i):
        return pltpu.make_async_copy(src, dst, lsem.at[i])

    c_wq = local(h_wq, wq, 0)
    c_wqr = local(h_wqr, wqr, 1)
    c_wl = local(h_wl, wl, 2)
    c_wkr = local(h_wkr, wkr, 3)
    c_wku = local(h_wku, wku, 4)
    c_wvu = local(h_wvu, wvu, 5)
    c_wo = local(h_wo, wo, 6)
    c_wg = local(h_wg.at[0], wg, 7)
    c_wu = local(h_wu.at[0], wu, 8)
    c_wd = local(h_wd.at[0], wd, 9)
    for c in (c_wku, c_wvu, c_wq, c_wqr, c_wl, c_wkr):
        c.start()

    def cache_copy(s):
        return pltpu.make_async_copy(h_clat.at[s], cache.at[s], csem.at[s])

    c_rope = pltpu.make_async_copy(h_crope, rope, rsem)

    def tp_copies(phase, src, dst):
        out = []
        for d in (2, 1, 3):
            j = (t + d) % TP
            out.append(
                pltpu.make_async_remote_copy(
                    src_ref=src(j),
                    dst_ref=dst,
                    send_sem=tss.at[phase, d],
                    recv_sem=trs.at[phase, d],
                    device_id={"tp": j},
                    device_id_type=MESH,
                )
            )
        return out

    tok32[...] = jnp.zeros((PAD, D), f32)
    tok32[0:SEQ, :] = tok_in[...].astype(f32)
    normed = rms(tok32[...], g_attn[...].astype(f32)).astype(bf16)
    nbuf[t] = normed
    pl.semaphore_wait(barrier, 34)
    ph0 = tp_copies(0, lambda j: nbuf.at[t], nbuf.at[t])
    for c in ph0:
        c.start()
    c_rope.start()
    for s in range(SEQ):
        cache_copy(s).start()
    for c in (c_wo, c_wg, c_wu, c_wd):
        c.start()

    r64[...] = jnp.full((TP * PAD, 4), -1, jnp.int32)
    l64[...] = jnp.zeros((TP * PAD, 4), f32)
    for j in range(TP):
        r64[PAD * j : PAD * j + SEQ, :] = routes_in[SEQ * j : SEQ * (j + 1), :]
        l64[PAD * j : PAD * j + SEQ, :] = logits_in[SEQ * j : SEQ * (j + 1), :]
    logits = l64[...]
    raised = jnp.exp(logits - jnp.max(logits, axis=-1, keepdims=True))
    rw = raised / jnp.sum(raised, axis=-1, keepdims=True)
    ids = r64[...]
    expert_of = lax.broadcasted_iota(jnp.int32, (TP * PAD, EP), 1)
    member = jnp.zeros((TP * PAD, EP), f32)
    weight = jnp.zeros((TP * PAD, EP), f32)
    for k in range(4):
        hit = ids[:, k : k + 1] == expert_of
        member = member + jnp.where(hit, 1.0, 0.0)
        weight = weight + jnp.where(hit, rw[:, k : k + 1], 0.0)
    lower = (
        lax.broadcasted_iota(jnp.int32, (TP * PAD, TP * PAD), 0)
        > lax.broadcasted_iota(jnp.int32, (TP * PAD, TP * PAD), 1)
    )
    member_b = member.astype(bf16)
    rank = mm(jnp.where(lower, 1.0, 0.0).astype(bf16), member_b)
    spread = jnp.where(
        lax.broadcasted_iota(jnp.int32, (EP, EP * CAPP), 1) // CAPP
        == lax.broadcasted_iota(jnp.int32, (EP, EP * CAPP), 0),
        1.0,
        0.0,
    ).astype(bf16)
    slot = (lax.broadcasted_iota(jnp.int32, (TP * PAD, EP * CAPP), 1) % CAPP).astype(f32)
    dt = jnp.where(
        (mm(member_b, spread) > 0.5) & (mm(rank.astype(bf16), spread) == slot), 1.0, 0.0
    )
    Dm[...] = jnp.transpose(dt).astype(bf16)
    w_hi = weight.astype(bf16)
    w_lo = (weight - w_hi.astype(f32)).astype(bf16)
    Cm[0 : TP * PAD, :] = (mm(w_hi, spread) * dt).astype(bf16)
    Cm[TP * PAD :, :] = (mm(w_lo, spread) * dt).astype(bf16)

    row = lax.broadcasted_iota(jnp.int32, (PAD, ROT), 0)
    col = lax.broadcasted_iota(jnp.int32, (PAD, ROT), 1)
    pos = jnp.zeros((PAD, ROT), f32)
    for s in range(SEQ):
        pos = jnp.where(row == s, lens[s].astype(f32), pos)
    half = ROT // 2
    freq = jnp.exp((col % half).astype(f32) * (-math.log(theta_base) / half))
    angle = pos * freq
    cosine = jnp.cos(angle)
    sine = jnp.where(col < half, -jnp.sin(angle), jnp.sin(angle))

    def rotate(v):
        swapped = jnp.concatenate([v[:, half:], v[:, :half]], axis=1)
        return v * cosine + swapped * sine

    c_wku.wait()
    c_wvu.wait()
    wtmp[0] = wku[...].astype(f32)
    wtmp[1] = wvu[...].astype(f32)
    for h in range(HL):
        wkh[h] = wtmp.at[0][pl.ds(h, LAT, stride=HL), :].astype(bf16)
        wvh[h] = wtmp.at[1][pl.ds(h, LAT, stride=HL), :].astype(bf16)

    c_wkr.wait()
    key_raw = mm(normed, wkr[...]).astype(bf16)
    new_rope = rotate(key_raw.astype(f32)).astype(bf16)
    rope_ref[...] = new_rope[0:SEQ]
    c_wq.wait()
    c_wqr.wait()
    c_wl.wait()
    for c in ph0:
        c.wait()

    rows = nbuf[...].reshape(TP * PAD, D)
    qp = mm(rows, wq[...]).astype(bf16)
    for h in range(HL):
        ql = mm_nt(qp[:, h * 128 : (h + 1) * 128], wkh[h]).astype(bf16)
        msg_s[:, :, h * LAT : (h + 1) * LAT] = ql.reshape(TP, PAD, LAT)
    msg_s[:, :, HL * LAT : HL * LAT + HL * ROT] = (
        mm(rows, wqr[...]).astype(bf16).reshape(TP, PAD, HL * ROT)
    )
    msg_s[:, :, HL * LAT + HL * ROT :] = mm(rows, wl[...]).astype(bf16).reshape(TP, PAD, 128)
    ph1 = tp_copies(1, lambda j: msg_s.at[j], msg_r.at[t])
    for c in ph1:
        c.start()
    msg_r[t] = msg_s[t]
    hl_s[...] = jnp.zeros((TP, HL, PAD, LAT), bf16)
    for c in ph1:
        c.wait()

    lat_raw = jnp.concatenate([msg_r[j, :, MSG - 128 :] for j in range(TP)], axis=1)
    new_latent = rms(lat_raw.astype(f32), g_lat[...].astype(f32)).astype(bf16)
    lat_ref[...] = new_latent[0:SEQ]
    nl32 = new_latent.astype(f32)
    nr32 = new_rope.astype(f32)
    scale = (128 + ROT) ** (-0.5)
    for j in range(TP):
        for h in range(HL):
            at = (j * HL + h) * PAD
            for c in range(LAT // 128):
                A[c, at : at + PAD, :] = msg_r[
                    j, :, h * LAT + c * 128 : h * LAT + (c + 1) * 128
                ].astype(f32)
            qr = msg_r[j, :, HL * LAT + h * ROT : HL * LAT + (h + 1) * ROT].astype(f32)
            A2[at : at + PAD, 0:ROT] = rotate(qr).astype(bf16).astype(f32)
            A2[at : at + PAD, ROT:] = jnp.zeros((PAD, 128 - ROT), f32)
    for s in range(SEQ):
        self_score = jnp.zeros((PAD, 128), f32)
        for c in range(LAT // 128):
            part = A.at[c][pl.ds(s, 16, stride=PAD), :]
            Q[s, :, c * 128 : (c + 1) * 128] = part.astype(bf16)
            self_score = self_score + part * nl32[s : s + 1, c * 128 : (c + 1) * 128]
        part = A2[pl.ds(s, 16, stride=PAD), :]
        Qr[s] = part.astype(bf16)
        total = jnp.sum(self_score, axis=-1, keepdims=True) + jnp.sum(
            part[:, 0:ROT] * nr32[s : s + 1, :], axis=-1, keepdims=True
        )
        ps_ref[s] = jnp.broadcast_to(total * scale, (16, 128))
    c_rope.wait()

    def score(s, carry):
        cache_copy(s).wait()
        val = mm_nt(Q[s], cache[s]) + mm(Qr[s, :, 0:ROT], rope[s])
        valid = lax.broadcasted_iota(jnp.int32, (16, LEN), 1) < lens[s]
        S[s] = jnp.where(valid, val * scale, -jnp.inf)
        return carry

    lax.fori_loop(0, SEQ, score, 0, unroll=2)

    def soft(s, carry):
        sc = S[s]
        own = ps_ref[s][:, 0:1]
        highest = jnp.maximum(jnp.max(sc, axis=-1, keepdims=True), own)
        e = jnp.exp(sc - highest)
        eo = jnp.exp(own - highest)
        total = jnp.sum(e, axis=-1, keepdims=True) + eo
        Pb[s] = (e / total).astype(bf16)
        ps_ref[s] = jnp.broadcast_to((eo / total).astype(bf16).astype(f32), (16, 128))
        return carry

    lax.fori_loop(0, SEQ, soft, 0, unroll=4)

    for s in range(SEQ):
        val = mm(Pb[s], cache[s]) + ps_ref[s][:, 0:1] * nl32[s : s + 1, :]
        for c in range(LAT // 128):
            O.at[c][pl.ds(s, 16, stride=PAD), :] = val[:, c * 128 : (c + 1) * 128]
    for j in range(TP):
        for h in range(HL):
            at = (j * HL + h) * PAD
            for c in range(LAT // 128):
                hl_s[j, h, 0:SEQ, c * 128 : (c + 1) * 128] = O[c, at : at + SEQ, :].astype(bf16)
    ph2 = tp_copies(2, lambda j: hl_s.at[j], hl_r.at[t])
    for c in ph2:
        c.start()
    hl_r[t] = hl_s[t]
    c_wo.wait()
    for c in ph2:
        c.wait()
    vals = jnp.concatenate(
        [mm(hl_r[:, h].reshape(TP * PAD, LAT), wvh[h]).astype(bf16) for h in range(HL)], axis=1
    )
    p_s[...] = mm(vals, wo[...]).astype(bf16).reshape(TP, PAD, D)
    ph3 = tp_copies(3, lambda j: p_s.at[j], p_r.at[t])
    for c in ph3:
        c.start()
    p_r[t] = p_s[t]
    for c in ph3:
        c.wait()
    attn = p_r[0].astype(f32)
    for j in range(1, TP):
        attn = attn + p_r[j].astype(f32)
    attn = attn.astype(bf16).astype(f32)
    mixed = (tok32[...] + rms(attn, g_post[...].astype(f32))).astype(bf16).astype(f32)
    mixed_ref[...] = mixed
    gbuf[t] = rms(mixed, g_ffn[...].astype(f32)).astype(bf16)
    ph4 = tp_copies(4, lambda j: gbuf.at[t], gbuf.at[t])
    for c in ph4:
        c.start()
    for c in (c_wg, c_wu, c_wd):
        c.wait()
    for c in ph4:
        c.wait()

    X[...] = mm(Dm[...], gbuf[...].reshape(TP * PAD, D)).astype(bf16).reshape(EP, CAPP, D)
    sent = []
    for d in far_first:
        e = ep_shift(me, d, 1)
        c = pltpu.make_async_remote_copy(
            src_ref=X.at[e],
            dst_ref=R.at[d],
            send_sem=dss.at[d],
            recv_sem=drs.at[d],
            device_id={"ep": e},
            device_id_type=MESH,
        )
        c.start()
        sent.append(c)
    R[0] = X[me]
    for c in sent:
        c.wait()
    flat = R[...].reshape(EP * CAPP, D)
    gate = jnp.minimum(mm(flat, wg[...]), clamp_limit)
    upward = jnp.clip(mm(flat, wu[...]), -clamp_limit, clamp_limit)
    active = ((upward + 1.0) * gate * jax.nn.sigmoid(sigmoid_alpha * gate)).astype(bf16)
    Y[...] = mm(active, wd[...]).astype(bf16).reshape(EP, CAPP, D)
    sent = []
    for d in far_first:
        c = pltpu.make_async_remote_copy(
            src_ref=Y.at[d],
            dst_ref=T.at[me],
            send_sem=ess.at[d],
            recv_sem=ers.at[d],
            device_id={"ep": ep_shift(me, d, -1)},
            device_id_type=MESH,
        )
        c.start()
        sent.append(c)
    T[me] = Y[0]
    for c in sent:
        c.wait()
    both = mm(Cm[...], T[...].reshape(EP * CAPP, D))
    m_s[...] = (both[0 : TP * PAD] + both[TP * PAD :]).astype(bf16).reshape(TP, PAD, D)
    ph5 = tp_copies(5, lambda j: m_s.at[j], m_r.at[t])
    for c in ph5:
        c.start()
    m_r[t] = m_s[t]
    for c in ph5:
        c.wait()
    moe = m_r[0].astype(f32)
    for j in range(1, TP):
        moe = moe + m_r[j].astype(f32)
    moe = moe.astype(bf16).astype(f32)
    res = (mixed_ref[...] + rms(moe, g_post2[...].astype(f32))).astype(bf16)
    out_ref[...] = res[0:SEQ]


def body(
    tokens,
    cache_latent,
    cache_rope,
    lengths,
    attn_gain,
    latent_gain,
    post_attn_gain,
    ffn_gain,
    post_ffn_gain,
    w_query,
    w_query_rot,
    w_latent,
    w_key_rot,
    w_key_up,
    w_value_up,
    w_out,
    route_logits,
    routes,
    w_gate,
    w_up,
    w_down,
):
    vm = pl.BlockSpec(memory_space=pltpu.VMEM)
    hbm = pl.BlockSpec(memory_space=pl.ANY)
    V = pltpu.VMEM
    scratch = [
        V((PAD, D), f32),
        V((TP, PAD, D), bf16),
        V((D, 512), bf16),
        V((D, 256), bf16),
        V((D, 128), bf16),
        V((D, ROT), bf16),
        V((HL * LAT, 128), bf16),
        V((HL * LAT, 128), bf16),
        V((2, HL * LAT, 128), f32),
        V((HL, LAT, 128), bf16),
        V((HL, LAT, 128), bf16),
        V((TP, PAD, MSG), bf16),
        V((TP, PAD, MSG), bf16),
        V((SEQ, LEN, LAT), bf16),
        V((SEQ, ROT, LEN), bf16),
        V((LAT // 128, 256, 128), f32),
        V((256, 128), f32),
        V((SEQ, 16, LAT), bf16),
        V((SEQ, 16, 128), bf16),
        V((SEQ, 16, LEN), f32),
        V((SEQ, 16, LEN), bf16),
        V((SEQ, 16, 128), f32),
        V((LAT // 128, 256, 128), f32),
        V((TP, HL, PAD, LAT), bf16),
        V((TP, HL, PAD, LAT), bf16),
        V((512, D), bf16),
        V((TP, PAD, D), bf16),
        V((TP, PAD, D), bf16),
        V((TP, PAD, D), bf16),
        V((PAD, D), f32),
        V((TP * PAD, 4), jnp.int32),
        V((TP * PAD, 4), f32),
        V((EP * CAPP, TP * PAD), bf16),
        V((2 * TP * PAD, EP * CAPP), bf16),
        V((EP, CAPP, D), bf16),
        V((EP, CAPP, D), bf16),
        V((EP, CAPP, D), bf16),
        V((EP, CAPP, D), bf16),
        V((D, 512), bf16),
        V((D, 512), bf16),
        V((512, D), bf16),
        V((TP, PAD, D), bf16),
        V((TP, PAD, D), bf16),
        pltpu.SemaphoreType.DMA((10,)),
        pltpu.SemaphoreType.DMA((SEQ,)),
        pltpu.SemaphoreType.DMA,
        pltpu.SemaphoreType.DMA((6, 4)),
        pltpu.SemaphoreType.DMA((6, 4)),
        pltpu.SemaphoreType.DMA((EP,)),
        pltpu.SemaphoreType.DMA((EP,)),
        pltpu.SemaphoreType.DMA((EP,)),
        pltpu.SemaphoreType.DMA((EP,)),
    ]
    return pl.pallas_call(
        layer_kernel,
        name="layer",
        out_shape=(
            jax.ShapeDtypeStruct((SEQ, D), bf16),
            jax.ShapeDtypeStruct((SEQ, LAT), bf16),
            jax.ShapeDtypeStruct((SEQ, ROT), bf16),
        ),
        in_specs=[pl.BlockSpec(memory_space=pltpu.SMEM)] + [vm] * 8 + [hbm] * 12,
        out_specs=(vm, vm, vm),
        scratch_shapes=scratch,
        compiler_params=pltpu.CompilerParams(
            collective_id=0, has_side_effects=True, vmem_limit_bytes=60 * 1024 * 1024
        ),
    )(
        lengths,
        tokens,
        routes,
        route_logits,
        attn_gain.reshape(1, -1),
        latent_gain.reshape(1, -1),
        post_attn_gain.reshape(1, -1),
        ffn_gain.reshape(1, -1),
        post_ffn_gain.reshape(1, -1),
        cache_latent,
        cache_rope,
        w_query,
        w_query_rot,
        w_latent,
        w_key_rot,
        w_key_up.reshape(-1, w_key_up.shape[2]),
        w_value_up.reshape(-1, w_value_up.shape[2]),
        w_out,
        w_gate,
        w_up,
        w_down,
    )


def solution(mesh):
    return jax.shard_map(
        body,
        mesh=mesh,
        in_specs=(
            P(("ep", "tp"), None),
            P(("ep", "tp"), None, None),
            P(("ep", "tp"), None, None),
            P(("ep", "tp")),
            P(),
            P(),
            P(),
            P(),
            P(),
            P(None, "tp"),
            P(None, "tp"),
            P(None, "tp"),
            P(),
            P(None, "tp", None),
            P(None, "tp", None),
            P("tp", None),
            P("ep", None),
            P("ep", None),
            P("ep", None, "tp"),
            P("ep", None, "tp"),
            P("ep", "tp", None),
        ),
        out_specs=(P(("ep", "tp"), None), P(("ep", "tp"), None), P(("ep", "tp"), None)),
        check_vma=False,
    )
```

```python
import functools
import math

import jax
import jax.numpy as jnp
from jax import lax
from jax.experimental import pallas as pl
from jax.experimental.pallas import tpu as pltpu
from jax.sharding import PartitionSpec as P

MESH = pl.DeviceIdType.MESH
eps_norm = 1e-06
clamp_limit = 7.0
sigmoid_alpha = 1.702
theta_base = 10000.0
f32 = jnp.float32
bf16 = jnp.bfloat16

SEQ = 12
PAD = 12
D = 2048
LAT = 512
ROT = 64
LEN = 1024
HL = 4
TP = 4
EP = 32
CAPP = 8
MSG = HL * LAT + HL * ROT + 128


def hops(a):
    return min(a, 4 - a)


far_first = sorted(range(1, EP), key=lambda d: -(hops(d // 8) + hops((d // 2) % 4)))


order = far_first + [0]
CHUNK = 16


def ep_shift(me, d, sign):
    z, y, c = me // 8, (me // 2) % 4, me % 2
    dz, dy, dc = d // 8, (d // 2) % 4, d % 2
    if sign < 0:
        dz, dy = (4 - dz) % 4, (4 - dy) % 4
    return ((z + dz) % 4) * 8 + ((y + dy) % 4) * 2 + (c + dc) % 2


def mm(a, b):
    return lax.dot_general(a, b, (((1,), (0,)), ((), ())), preferred_element_type=f32)


def mm_nt(a, b):
    return lax.dot_general(a, b, (((1,), (1,)), ((), ())), preferred_element_type=f32)


def rms(v, gain):
    mean_square = jnp.mean(v * v, axis=-1, keepdims=True)
    return v * lax.rsqrt(mean_square + eps_norm) * gain


def layer_kernel(
    h_lens,
    h_tok,
    h_routes,
    h_logits,
    h_attn,
    h_lat,
    h_post,
    h_ffn,
    h_post2,
    h_clat,
    h_crope,
    h_wq,
    h_wqr,
    h_wl,
    h_wkr,
    h_wku,
    h_wvu,
    h_wo,
    h_wg,
    h_wu,
    h_wd,
    out_ref,
    lat_ref,
    rope_ref,
    lens,
    tok_in,
    routes_in,
    logits_in,
    g_attn,
    g_lat,
    g_post,
    g_ffn,
    g_post2,
    tok32,
    nbuf,
    wq,
    wqr,
    wl,
    wkr,
    wku,
    wvu,
    wtmp,
    wkh,
    wvh,
    msg_s,
    msg_r,
    cache,
    rope,
    A,
    A2,
    Q,
    Qr,
    S,
    Pb,
    ps_ref,
    O,
    hl_s,
    hl_r,
    wo,
    p_s,
    p_r,
    gbuf,
    mixed_ref,
    Dm,
    Cm,
    X,
    R,
    Y,
    T,
    wg,
    wu,
    wd,
    m_s,
    m_r,
    lsem,
    csem,
    rsem,
    tss,
    trs,
    dss,
    drs,
    ess,
    ers,
):
    me = lax.axis_index("ep")
    t = lax.axis_index("tp")
    barrier = pltpu.get_barrier_semaphore()
    for d in (1, 2, 3):
        pl.semaphore_signal(barrier, inc=1, device_id={"tp": (t + d) % TP}, device_id_type=MESH)
    for d in far_first:
        pl.semaphore_signal(barrier, inc=1, device_id={"ep": ep_shift(me, d, 1)}, device_id_type=MESH)

    def local(src, dst, i):
        return pltpu.make_async_copy(src, dst, lsem.at[i])

    c_wq = local(h_wq, wq, 0)
    c_wqr = local(h_wqr, wqr, 1)
    c_wl = local(h_wl, wl, 2)
    c_wkr = local(h_wkr, wkr, 3)
    c_wku = local(h_wku, wku, 4)
    c_wvu = local(h_wvu, wvu, 5)
    c_wo = local(h_wo, wo, 6)
    c_wg = local(h_wg.at[0], wg, 7)
    c_wu = local(h_wu.at[0], wu, 8)
    c_wd = local(h_wd.at[0], wd, 9)
    c_tok = local(h_tok, tok_in, 10)
    c_attn = local(h_attn, g_attn, 11)
    c_lens = local(h_lens, lens, 12)
    c_routes = local(h_routes, routes_in, 13)
    c_logits = local(h_logits, logits_in, 14)
    c_lat = local(h_lat, g_lat, 15)
    c_post = local(h_post, g_post, 16)
    c_ffn = local(h_ffn, g_ffn, 17)
    c_post2 = local(h_post2, g_post2, 18)
    small = (c_lens, c_routes, c_logits, c_lat, c_post, c_ffn, c_post2)
    for c in (c_tok, c_attn) + small + (c_wku, c_wvu, c_wq, c_wqr, c_wl, c_wkr):
        c.start()

    def cache_copy(s):
        return pltpu.make_async_copy(h_clat.at[s], cache.at[s], csem.at[s])

    c_rope = pltpu.make_async_copy(h_crope, rope, rsem)

    c_rope.start()
    for s in range(SEQ):
        cache_copy(s).start()

    def tp_copies(phase, src, dst):
        out = []
        for d in (2, 1, 3):
            j = (t + d) % TP
            out.append(
                pltpu.make_async_remote_copy(
                    src_ref=src(j),
                    dst_ref=dst,
                    send_sem=tss.at[phase, d],
                    recv_sem=trs.at[phase, d],
                    device_id={"tp": j},
                    device_id_type=MESH,
                )
            )
        return out

    c_tok.wait()
    c_attn.wait()
    tok32[...] = tok_in[...].astype(f32)
    normed = rms(tok32[...], g_attn[...].astype(f32)).astype(bf16)
    nbuf[t] = normed.reshape(3, 4, D)
    with jax.named_scope("wait_barrier"):
        pl.semaphore_wait(barrier, 34)
    ph0 = tp_copies(0, lambda j: nbuf.at[t], nbuf.at[t])
    for c in ph0:
        c.start()

    for c in small:
        c.wait()

    logits = logits_in[...]
    raised = jnp.exp(logits - jnp.max(logits, axis=0, keepdims=True))
    rw = raised / jnp.sum(raised, axis=0, keepdims=True)
    ids = routes_in[...]
    expert_of = lax.broadcasted_iota(jnp.int32, (EP, TP * PAD), 0)
    member = jnp.zeros((EP, TP * PAD), f32)
    weight = jnp.zeros((EP, TP * PAD), f32)
    for k in range(4):
        hit = ids[k : k + 1, :] == expert_of
        member = member + jnp.where(hit, 1.0, 0.0)
        weight = weight + jnp.where(hit, rw[k : k + 1, :], 0.0)
    earlier = (
        lax.broadcasted_iota(jnp.int32, (TP * PAD, TP * PAD), 0)
        < lax.broadcasted_iota(jnp.int32, (TP * PAD, TP * PAD), 1)
    )
    member_b = member.astype(bf16)
    rank = mm(member_b, jnp.where(earlier, 1.0, 0.0).astype(bf16))
    spread = jnp.where(
        lax.broadcasted_iota(jnp.int32, (EP * CAPP, EP), 0) // CAPP
        == lax.broadcasted_iota(jnp.int32, (EP * CAPP, EP), 1),
        1.0,
        0.0,
    ).astype(bf16)
    slot = (lax.broadcasted_iota(jnp.int32, (EP * CAPP, TP * PAD), 0) % CAPP).astype(f32)
    dm = jnp.where(
        (mm(spread, member_b) > 0.5) & (mm(spread, rank.astype(bf16)) == slot), 1.0, 0.0
    )
    Dm[...] = dm.astype(bf16)
    w_hi = weight.astype(bf16)
    w_lo = (weight - w_hi.astype(f32)).astype(bf16)
    Cm[0 : TP * PAD, :] = jnp.transpose(mm(spread, w_hi) * dm).astype(bf16)
    Cm[TP * PAD :, :] = jnp.transpose(mm(spread, w_lo) * dm).astype(bf16)

    row = lax.broadcasted_iota(jnp.int32, (PAD, ROT), 0)
    col = lax.broadcasted_iota(jnp.int32, (PAD, ROT), 1)
    pos = jnp.zeros((PAD, ROT), f32)
    for s in range(SEQ):
        pos = jnp.where(row == s, lens[s].astype(f32), pos)
    half = ROT // 2
    freq = jnp.exp((col % half).astype(f32) * (-math.log(theta_base) / half))
    angle = pos * freq
    cosine = jnp.cos(angle)
    sine = jnp.where(col < half, -jnp.sin(angle), jnp.sin(angle))

    def rotate(v):
        swapped = jnp.concatenate([v[:, half:], v[:, :half]], axis=1)
        return v * cosine + swapped * sine

    with jax.named_scope("wait_up"):
        c_wku.wait()
        c_wvu.wait()
    wtmp[0] = wku[...].astype(f32)
    wtmp[1] = wvu[...].astype(f32)
    for h in range(HL):
        wkh[h] = wtmp.at[0][pl.ds(h, LAT, stride=HL), :].astype(bf16)
        wvh[h] = wtmp.at[1][pl.ds(h, LAT, stride=HL), :].astype(bf16)

    c_wkr.wait()
    key_raw = mm_nt(normed, wkr[...]).astype(bf16)
    new_rope = rotate(key_raw.astype(f32)).astype(bf16)
    rope_ref[...] = new_rope
    with jax.named_scope("wait_wq"):
        c_wq.wait()
        c_wqr.wait()
        c_wl.wait()
    with jax.named_scope("wait_tp0"):
        for c in ph0:
            c.wait()

    rows = nbuf[...].reshape(TP * PAD, D)
    qp = mm(rows, wq[...]).astype(bf16)
    for h in range(HL):
        ql = mm_nt(qp[:, h * 128 : (h + 1) * 128], wkh[h]).astype(bf16)
        msg_s[:, :, :, h * LAT : (h + 1) * LAT] = ql.reshape(TP, 3, 4, LAT)
    msg_s[:, :, :, HL * LAT : HL * LAT + HL * ROT] = (
        mm(rows, wqr[...]).astype(bf16).reshape(TP, 3, 4, HL * ROT)
    )
    msg_s[:, :, :, HL * LAT + HL * ROT :] = (
        mm(rows, wl[...]).astype(bf16).reshape(TP, 3, 4, 128)
    )
    ph1 = tp_copies(1, lambda j: msg_s.at[j], msg_r.at[t])
    for c in ph1:
        c.start()
    msg_r[t] = msg_s[t]
    with jax.named_scope("wait_tp1"):
        for c in ph1:
            c.wait()

    lat_raw = jnp.concatenate([msg_r[j, :, :, MSG - 128 :].reshape(PAD, 128) for j in range(TP)], axis=1)
    new_latent = rms(lat_raw.astype(f32), g_lat[...].astype(f32)).astype(bf16)
    lat_ref[...] = new_latent
    nl32 = new_latent.astype(f32)
    nr32 = new_rope.astype(f32)
    scale = (128 + ROT) ** (-0.5)
    for j in range(TP):
        for h in range(HL):
            at = (j * HL + h) * PAD
            for c in range(LAT // 128):
                A[c, at : at + PAD, :] = (
                    msg_r[j, :, :, h * LAT + c * 128 : h * LAT + (c + 1) * 128]
                    .reshape(PAD, 128)
                    .astype(f32)
                )
            qr = (
                msg_r[j, :, :, HL * LAT + h * ROT : HL * LAT + (h + 1) * ROT]
                .reshape(PAD, ROT)
                .astype(f32)
            )
            A2[at : at + PAD, 0:ROT] = rotate(qr).astype(bf16).astype(f32)
            A2[at : at + PAD, ROT:] = jnp.zeros((PAD, 128 - ROT), f32)
    for s in range(SEQ):
        self_score = jnp.zeros((16, 128), f32)
        for c in range(LAT // 128):
            part = A.at[c][pl.ds(s, 16, stride=PAD), :]
            Q[s, :, c * 128 : (c + 1) * 128] = part.astype(bf16)
            self_score = self_score + part * nl32[s : s + 1, c * 128 : (c + 1) * 128]
        part = A2[pl.ds(s, 16, stride=PAD), :]
        Qr[s] = part.astype(bf16)
        total = jnp.sum(self_score, axis=-1, keepdims=True) + jnp.sum(
            part[:, 0:ROT] * nr32[s : s + 1, :], axis=-1, keepdims=True
        )
        ps_ref[s] = jnp.broadcast_to(total * scale, (16, 128))
    c_rope.wait()

    def score(s, carry):
        cache_copy(s).wait()
        val = mm_nt(Q[s], cache[s]) + mm(Qr[s, :, 0:ROT], rope[s])
        valid = lax.broadcasted_iota(jnp.int32, (16, LEN), 1) < lens[s]
        S[s] = jnp.where(valid, val * scale, -jnp.inf)
        return carry

    with jax.named_scope("scores"):
        lax.fori_loop(0, SEQ, score, 0, unroll=2)

    def soft(s, carry):
        sc = S[s]
        own = ps_ref[s][:, 0:1]
        highest = jnp.maximum(jnp.max(sc, axis=-1, keepdims=True), own)
        e = jnp.exp(sc - highest)
        eo = jnp.exp(own - highest)
        total = jnp.sum(e, axis=-1, keepdims=True) + eo
        Pb[s] = (e / total).astype(bf16)
        ps_ref[s] = jnp.broadcast_to((eo / total).astype(bf16).astype(f32), (16, 128))
        return carry

    for c in (c_wo, c_wg, c_wu, c_wd):
        c.start()
    with jax.named_scope("softmax"):
        lax.fori_loop(0, SEQ, soft, 0, unroll=4)

    for s in range(SEQ):
        val = mm(Pb[s], cache[s]) + ps_ref[s][:, 0:1] * nl32[s : s + 1, :]
        for c in range(LAT // 128):
            O.at[c][pl.ds(s, 16, stride=PAD), :] = val[:, c * 128 : (c + 1) * 128]
    for j in range(TP):
        for h in range(HL):
            at = (j * HL + h) * PAD
            for c in range(LAT // 128):
                hl_s[j, h, :, :, c * 128 : (c + 1) * 128] = (
                    O[c, at : at + PAD, :].astype(bf16).reshape(3, 4, 128)
                )
    ph2 = tp_copies(2, lambda j: hl_s.at[j], hl_r.at[t])
    for c in ph2:
        c.start()
    hl_r[t] = hl_s[t]
    c_wo.wait()
    with jax.named_scope("wait_tp2"):
        for c in ph2:
            c.wait()
    vals = jnp.concatenate(
        [mm(hl_r[:, h].reshape(TP * PAD, LAT), wvh[h]).astype(bf16) for h in range(HL)], axis=1
    )
    p_s[...] = mm(vals, wo[...]).astype(bf16).reshape(TP, 3, 4, D)
    ph3 = tp_copies(3, lambda j: p_s.at[j], p_r.at[t])
    for c in ph3:
        c.start()
    p_r[t] = p_s[t]
    with jax.named_scope("wait_tp3"):
        for c in ph3:
            c.wait()
    attn = p_r[0].reshape(PAD, D).astype(f32)
    for j in range(1, TP):
        attn = attn + p_r[j].reshape(PAD, D).astype(f32)
    attn = attn.astype(bf16).astype(f32)
    mixed = (tok32[...] + rms(attn, g_post[...].astype(f32))).astype(bf16).astype(f32)
    mixed_ref[...] = mixed
    gbuf[t] = rms(mixed, g_ffn[...].astype(f32)).astype(bf16).reshape(3, 4, D)
    ph4 = tp_copies(4, lambda j: gbuf.at[t], gbuf.at[t])
    for c in ph4:
        c.start()
    for c in (c_wg, c_wu, c_wd):
        c.wait()
    with jax.named_scope("wait_tp4"):
        for c in ph4:
            c.wait()

    X[...] = mm(Dm[...], gbuf[...].reshape(TP * PAD, D)).astype(bf16).reshape(EP, CAPP, D)
    for p, d in enumerate(order):
        if d:
            e = ep_shift(me, d, 1)
            pltpu.make_async_remote_copy(
                src_ref=X.at[e],
                dst_ref=R.at[p],
                send_sem=dss,
                recv_sem=drs.at[p // CHUNK],
                device_id={"ep": e},
                device_id_type=MESH,
            ).start()
        else:
            R[p] = X[me]

    def arrived(ref, sem):
        pltpu.make_async_copy(ref, ref, sem).wait()

    for k in range(EP // CHUNK):
        lo, hi = k * CHUNK, (k + 1) * CHUNK
        with jax.named_scope(f"wait_dispatch{k}"):
            arrived(R.at[lo : min(hi, EP - 1)], drs.at[k])
        flat = R[lo:hi].reshape(CHUNK * CAPP, D)
        gate = jnp.minimum(mm(flat, wg[...]), clamp_limit)
        upward = jnp.clip(mm(flat, wu[...]), -clamp_limit, clamp_limit)
        active = ((upward + 1.0) * gate * jax.nn.sigmoid(sigmoid_alpha * gate)).astype(bf16)
        Y[lo:hi] = mm(active, wd[...]).astype(bf16).reshape(CHUNK, CAPP, D)
        for p in range(lo, hi):
            d = order[p]
            if d:
                pltpu.make_async_remote_copy(
                    src_ref=Y.at[p],
                    dst_ref=T.at[me],
                    send_sem=ess,
                    recv_sem=ers,
                    device_id={"ep": ep_shift(me, d, -1)},
                    device_id_type=MESH,
                ).start()
            else:
                T[me] = Y[p]
    with jax.named_scope("wait_return"):
        arrived(T.at[0 : EP - 1], ers)
    both = mm(Cm[...], T[...].reshape(EP * CAPP, D))
    m_s[...] = (both[0 : TP * PAD] + both[TP * PAD :]).astype(bf16).reshape(TP, 3, 4, D)
    ph5 = tp_copies(5, lambda j: m_s.at[j], m_r.at[t])
    for c in ph5:
        c.start()
    m_r[t] = m_s[t]
    with jax.named_scope("wait_tp5"):
        for c in ph5:
            c.wait()
    with jax.named_scope("final"):
      moe = m_r[0].reshape(PAD, D).astype(f32)
      for j in range(1, TP):
        moe = moe + m_r[j].reshape(PAD, D).astype(f32)
      moe = moe.astype(bf16).astype(f32)
      arrived(X.at[0 : EP - 1], dss)
      arrived(Y.at[0 : EP - 1], ess)
      res = (mixed_ref[...] + rms(moe, g_post2[...].astype(f32))).astype(bf16)
      out_ref[...] = res


def finish_kernel(a, b, c, x, y, z, sem):
    copies = [pltpu.make_async_copy(p, q, sem.at[i]) for i, (p, q) in enumerate(((a, x), (b, y), (c, z)))]
    for p in copies:
        p.start()
    for p in copies:
        p.wait()


def body(
    tokens,
    cache_latent,
    cache_rope,
    lengths,
    attn_gain,
    latent_gain,
    post_attn_gain,
    ffn_gain,
    post_ffn_gain,
    w_query,
    w_query_rot,
    w_latent,
    w_key_rot,
    w_key_up,
    w_value_up,
    w_out,
    route_logits,
    routes,
    w_gate,
    w_up,
    w_down,
):
    vm = pl.BlockSpec(memory_space=pltpu.VMEM)
    hbm = pl.BlockSpec(memory_space=pl.ANY)
    V = pltpu.VMEM
    scratch = [
        pltpu.SMEM((SEQ,), jnp.int32),
        V((SEQ, D), bf16),
        V((4, TP * SEQ), jnp.int32),
        V((4, TP * SEQ), f32),
        V((D,), bf16),
        V((LAT,), bf16),
        V((D,), bf16),
        V((D,), bf16),
        V((D,), bf16),
        V((PAD, D), f32),
        V((TP, 3, 4, D), bf16),
        V((D, 512), bf16),
        V((D, 256), bf16),
        V((D, 128), bf16),
        V((ROT, D), bf16),
        V((HL * LAT, 128), bf16),
        V((HL * LAT, 128), bf16),
        V((2, HL * LAT, 128), f32),
        V((HL, LAT, 128), bf16),
        V((HL, LAT, 128), bf16),
        V((TP, 3, 4, MSG), bf16),
        V((TP, 3, 4, MSG), bf16),
        V((SEQ, LEN, LAT), bf16),
        V((SEQ, ROT, LEN), bf16),
        V((LAT // 128, 16 * PAD, 128), f32),
        V((16 * PAD, 128), f32),
        V((SEQ, 16, LAT), bf16),
        V((SEQ, 16, 128), bf16),
        V((SEQ, 16, LEN), f32),
        V((SEQ, 16, LEN), bf16),
        V((SEQ, 16, 128), f32),
        V((LAT // 128, 16 * PAD, 128), f32),
        V((TP, HL, 3, 4, LAT), bf16),
        V((TP, HL, 3, 4, LAT), bf16),
        V((512, D), bf16),
        V((TP, 3, 4, D), bf16),
        V((TP, 3, 4, D), bf16),
        V((TP, 3, 4, D), bf16),
        V((PAD, D), f32),
        V((EP * CAPP, TP * PAD), bf16),
        V((2 * TP * PAD, EP * CAPP), bf16),
        V((EP, CAPP, D), bf16),
        V((EP, CAPP, D), bf16),
        V((EP, CAPP, D), bf16),
        V((EP, CAPP, D), bf16),
        V((D, 512), bf16),
        V((D, 512), bf16),
        V((512, D), bf16),
        V((TP, 3, 4, D), bf16),
        V((TP, 3, 4, D), bf16),
        pltpu.SemaphoreType.DMA((19,)),
        pltpu.SemaphoreType.DMA((SEQ,)),
        pltpu.SemaphoreType.DMA,
        pltpu.SemaphoreType.DMA((6, 4)),
        pltpu.SemaphoreType.DMA((6, 4)),
        pltpu.SemaphoreType.DMA,
        pltpu.SemaphoreType.DMA((EP // CHUNK,)),
        pltpu.SemaphoreType.DMA,
        pltpu.SemaphoreType.DMA,
    ]
    parts = pl.pallas_call(
        layer_kernel,
        name="layer",
        out_shape=(
            pltpu.VMEM((SEQ, D), bf16),
            pltpu.VMEM((SEQ, LAT), bf16),
            pltpu.VMEM((SEQ, ROT), bf16),
        ),
        in_specs=[hbm] * 21,
        out_specs=(vm, vm, vm),
        scratch_shapes=scratch,
        compiler_params=pltpu.CompilerParams(
            collective_id=0, has_side_effects=True, vmem_limit_bytes=60 * 1024 * 1024
        ),
    )(
        lengths,
        tokens,
        routes.T,
        route_logits.T,
        attn_gain,
        latent_gain,
        post_attn_gain,
        ffn_gain,
        post_ffn_gain,
        cache_latent,
        cache_rope,
        w_query,
        w_query_rot,
        w_latent,
        w_key_rot.T,
        w_key_up.reshape(-1, w_key_up.shape[2]),
        w_value_up.reshape(-1, w_value_up.shape[2]),
        w_out,
        w_gate,
        w_up,
        w_down,
    )
    parts = [pltpu.with_memory_space_constraint(p, pltpu.VMEM) for p in parts]
    return pl.pallas_call(
        finish_kernel,
        name="finish",
        out_shape=(
            jax.ShapeDtypeStruct((SEQ, D), bf16),
            jax.ShapeDtypeStruct((SEQ, LAT), bf16),
            jax.ShapeDtypeStruct((SEQ, ROT), bf16),
        ),
        in_specs=[vm] * 3,
        out_specs=(hbm,) * 3,
        scratch_shapes=[pltpu.SemaphoreType.DMA((3,))],
    )(*parts)


def solution(mesh):
    return jax.shard_map(
        body,
        mesh=mesh,
        in_specs=(
            P(("ep", "tp"), None),
            P(("ep", "tp"), None, None),
            P(("ep", "tp"), None, None),
            P(("ep", "tp")),
            P(),
            P(),
            P(),
            P(),
            P(),
            P(None, "tp"),
            P(None, "tp"),
            P(None, "tp"),
            P(),
            P(None, "tp", None),
            P(None, "tp", None),
            P("tp", None),
            P("ep", None),
            P("ep", None),
            P("ep", None, "tp"),
            P("ep", None, "tp"),
            P("ep", "tp", None),
        ),
        out_specs=(P(("ep", "tp"), None), P(("ep", "tp"), None), P(("ep", "tp"), None)),
        check_vma=False,
    )
```

```python
import functools
import math

import jax
import jax.numpy as jnp
from jax import lax
from jax.experimental import pallas as pl
from jax.experimental.pallas import tpu as pltpu
from jax.sharding import PartitionSpec as P

MESH = pl.DeviceIdType.MESH
eps_norm = 1e-06
clamp_limit = 7.0
sigmoid_alpha = 1.702
theta_base = 10000.0
f32 = jnp.float32
bf16 = jnp.bfloat16

SEQ = 12
PAD = 12
D = 2048
LAT = 512
ROT = 64
LEN = 1024
HL = 4
TP = 4
EP = 32
CAPP = 8
MSG = HL * LAT + HL * ROT + 128


def hops(a):
    return min(a, 4 - a)


far_first = sorted(range(1, EP), key=lambda d: -(hops(d // 8) + hops((d // 2) % 4)))


order = far_first + [0]
CHUNK = 16


def ep_shift(me, d, sign):
    z, y, c = me // 8, (me // 2) % 4, me % 2
    dz, dy, dc = d // 8, (d // 2) % 4, d % 2
    if sign < 0:
        dz, dy = (4 - dz) % 4, (4 - dy) % 4
    return ((z + dz) % 4) * 8 + ((y + dy) % 4) * 2 + (c + dc) % 2


def mm(a, b):
    return lax.dot_general(a, b, (((1,), (0,)), ((), ())), preferred_element_type=f32)


def mm_nt(a, b):
    return lax.dot_general(a, b, (((1,), (1,)), ((), ())), preferred_element_type=f32)


def rms(v, gain):
    mean_square = jnp.mean(v * v, axis=-1, keepdims=True)
    return v * lax.rsqrt(mean_square + eps_norm) * gain


def layer_kernel(
    h_lens,
    h_tok,
    h_routes,
    h_logits,
    h_attn,
    h_lat,
    h_post,
    h_ffn,
    h_post2,
    h_clat,
    h_crope,
    h_wq,
    h_wqr,
    h_wl,
    h_wkr,
    h_wku,
    h_wvu,
    h_wo,
    h_wg,
    h_wu,
    h_wd,
    out_ref,
    lat_ref,
    rope_ref,
    lens,
    tok_in,
    routes_in,
    logits_in,
    g_attn,
    g_lat,
    g_post,
    g_ffn,
    g_post2,
    tok32,
    nbuf,
    wq,
    wqr,
    wl,
    wkr,
    wku,
    wvu,
    wtmp,
    wkh,
    wvh,
    msg_s,
    msg_r,
    cache,
    turned,
    rope,
    A,
    A2,
    Q,
    Qr,
    S,
    Pb,
    ps_ref,
    O,
    hl_s,
    hl_r,
    wo,
    p_s,
    p_r,
    gbuf,
    mixed_ref,
    Dm,
    Cm,
    X,
    R,
    Y,
    T,
    wg,
    wu,
    wd,
    m_s,
    m_r,
    lsem,
    csem,
    rsem,
    tss,
    trs,
    hss,
    hrs,
    dss,
    drs,
    ess,
    ers,
):
    me = lax.axis_index("ep")
    t = lax.axis_index("tp")
    barrier = pltpu.get_barrier_semaphore()
    for d in (1, 2, 3):
        pl.semaphore_signal(barrier, inc=1, device_id={"tp": (t + d) % TP}, device_id_type=MESH)
    for d in far_first:
        pl.semaphore_signal(barrier, inc=1, device_id={"ep": ep_shift(me, d, 1)}, device_id_type=MESH)

    def local(src, dst, i):
        return pltpu.make_async_copy(src, dst, lsem.at[i])

    c_wq = local(h_wq, wq, 0)
    c_wqr = local(h_wqr, wqr, 1)
    c_wl = local(h_wl, wl, 2)
    c_wkr = local(h_wkr, wkr, 3)
    c_wku = local(h_wku, wku, 4)
    c_wvu = local(h_wvu, wvu, 5)
    c_wo = local(h_wo, wo, 6)
    c_wg = local(h_wg.at[0], wg, 7)
    c_wu = local(h_wu.at[0], wu, 8)
    c_wd = local(h_wd.at[0], wd, 9)
    c_tok = local(h_tok, tok_in, 10)
    c_attn = local(h_attn, g_attn, 11)
    c_lens = local(h_lens, lens, 12)
    c_routes = local(h_routes, routes_in, 13)
    c_logits = local(h_logits, logits_in, 14)
    c_lat = local(h_lat, g_lat, 15)
    c_post = local(h_post, g_post, 16)
    c_ffn = local(h_ffn, g_ffn, 17)
    c_post2 = local(h_post2, g_post2, 18)
    small = (c_lens, c_routes, c_logits, c_lat, c_post, c_ffn, c_post2)
    for c in (c_tok, c_attn) + small + (c_wku, c_wvu, c_wq, c_wqr, c_wl, c_wkr):
        c.start()

    def cache_copy(s):
        return pltpu.make_async_copy(h_clat.at[s], cache.at[s], csem.at[s])

    c_rope = pltpu.make_async_copy(h_crope, rope, rsem)

    c_rope.start()
    for s in range(SEQ):
        cache_copy(s).start()

    def arrived(ref, sem):
        pltpu.make_async_copy(ref, ref, sem).wait()

    def turn(s):
        cache_copy(s).wait()
        turned[s] = cache[s].T

    def tp_copies(phase, src, dst):
        out = []
        for d in (2, 1, 3):
            j = (t + d) % TP
            out.append(
                pltpu.make_async_remote_copy(
                    src_ref=src(j),
                    dst_ref=dst,
                    send_sem=tss.at[phase, d],
                    recv_sem=trs.at[phase, d],
                    device_id={"tp": j},
                    device_id_type=MESH,
                )
            )
        return out

    c_tok.wait()
    c_attn.wait()
    tok32[...] = tok_in[...].astype(f32)
    normed = rms(tok32[...], g_attn[...].astype(f32)).astype(bf16)
    nbuf[t] = normed.reshape(3, 4, D)
    with jax.named_scope("wait_barrier"):
        pl.semaphore_wait(barrier, 34)
    ph0 = tp_copies(0, lambda j: nbuf.at[t], nbuf.at[t])
    for c in ph0:
        c.start()

    for c in small:
        c.wait()

    logits = logits_in[...]
    raised = jnp.exp(logits - jnp.max(logits, axis=0, keepdims=True))
    rw = raised / jnp.sum(raised, axis=0, keepdims=True)
    ids = routes_in[...]
    place = lax.broadcasted_iota(jnp.int32, (EP, TP * PAD), 0)
    expert_of = jnp.zeros((EP, TP * PAD), jnp.int32)
    for p, d in enumerate(order):
        expert_of = jnp.where(place == p, ep_shift(me, d, 1), expert_of)
    member = jnp.zeros((EP, TP * PAD), f32)
    weight = jnp.zeros((EP, TP * PAD), f32)
    for k in range(4):
        hit = ids[k : k + 1, :] == expert_of
        member = member + jnp.where(hit, 1.0, 0.0)
        weight = weight + jnp.where(hit, rw[k : k + 1, :], 0.0)
    earlier = (
        lax.broadcasted_iota(jnp.int32, (TP * PAD, TP * PAD), 0)
        < lax.broadcasted_iota(jnp.int32, (TP * PAD, TP * PAD), 1)
    )
    member_b = member.astype(bf16)
    rank = mm(member_b, jnp.where(earlier, 1.0, 0.0).astype(bf16))
    spread = jnp.where(
        lax.broadcasted_iota(jnp.int32, (EP * CAPP, EP), 0) // CAPP
        == lax.broadcasted_iota(jnp.int32, (EP * CAPP, EP), 1),
        1.0,
        0.0,
    ).astype(bf16)
    slot = (lax.broadcasted_iota(jnp.int32, (EP * CAPP, TP * PAD), 0) % CAPP).astype(f32)
    dm = jnp.where(
        (mm(spread, member_b) > 0.5) & (mm(spread, rank.astype(bf16)) == slot), 1.0, 0.0
    )
    Dm[...] = dm.astype(bf16)
    w_hi = weight.astype(bf16)
    w_lo = (weight - w_hi.astype(f32)).astype(bf16)
    Cm[0 : TP * PAD, :] = jnp.transpose(mm(spread, w_hi) * dm).astype(bf16)
    Cm[TP * PAD :, :] = jnp.transpose(mm(spread, w_lo) * dm).astype(bf16)

    row = lax.broadcasted_iota(jnp.int32, (PAD, ROT), 0)
    col = lax.broadcasted_iota(jnp.int32, (PAD, ROT), 1)
    pos = jnp.zeros((PAD, ROT), f32)
    for s in range(SEQ):
        pos = jnp.where(row == s, lens[s].astype(f32), pos)
    half = ROT // 2
    freq = jnp.exp((col % half).astype(f32) * (-math.log(theta_base) / half))
    angle = pos * freq
    cosine = jnp.cos(angle)
    sine = jnp.where(col < half, -jnp.sin(angle), jnp.sin(angle))

    def rotate(v):
        swapped = jnp.concatenate([v[:, half:], v[:, :half]], axis=1)
        return v * cosine + swapped * sine

    with jax.named_scope("wait_up"):
        c_wku.wait()
        c_wvu.wait()
    wtmp[0] = wku[...].astype(f32)
    wtmp[1] = wvu[...].astype(f32)
    for h in range(HL):
        wkh[h] = wtmp.at[0][pl.ds(h, LAT, stride=HL), :].astype(bf16)
        wvh[h] = wtmp.at[1][pl.ds(h, LAT, stride=HL), :].astype(bf16)

    c_wkr.wait()
    key_raw = mm_nt(normed, wkr[...]).astype(bf16)
    new_rope = rotate(key_raw.astype(f32)).astype(bf16)
    rope_ref[...] = new_rope
    with jax.named_scope("turn0"):
        for s in range(4):
            turn(s)
    with jax.named_scope("wait_wq"):
        c_wq.wait()
        c_wqr.wait()
        c_wl.wait()
    with jax.named_scope("wait_tp0"):
        for c in ph0:
            c.wait()

    rows = nbuf[...].reshape(TP * PAD, D)
    qp = mm(rows, wq[...]).astype(bf16)
    for h in range(HL):
        ql = mm_nt(qp[:, h * 128 : (h + 1) * 128], wkh[h]).astype(bf16)
        msg_s[:, :, :, h * LAT : (h + 1) * LAT] = ql.reshape(TP, 3, 4, LAT)
    msg_s[:, :, :, HL * LAT : HL * LAT + HL * ROT] = (
        mm(rows, wqr[...]).astype(bf16).reshape(TP, 3, 4, HL * ROT)
    )
    msg_s[:, :, :, HL * LAT + HL * ROT :] = (
        mm(rows, wl[...]).astype(bf16).reshape(TP, 3, 4, 128)
    )
    ph1 = tp_copies(1, lambda j: msg_s.at[j], msg_r.at[t])
    for c in ph1:
        c.start()
    msg_r[t] = msg_s[t]
    with jax.named_scope("turn1"):
        for s in range(4, SEQ):
            turn(s)
    with jax.named_scope("wait_tp1"):
        for c in ph1:
            c.wait()

    lat_raw = jnp.concatenate([msg_r[j, :, :, MSG - 128 :].reshape(PAD, 128) for j in range(TP)], axis=1)
    new_latent = rms(lat_raw.astype(f32), g_lat[...].astype(f32)).astype(bf16)
    lat_ref[...] = new_latent
    nl32 = new_latent.astype(f32)
    nr32 = new_rope.astype(f32)
    scale = (128 + ROT) ** (-0.5)
    for j in range(TP):
        for h in range(HL):
            at = (j * HL + h) * PAD
            for c in range(LAT // 128):
                A[c, at : at + PAD, :] = (
                    msg_r[j, :, :, h * LAT + c * 128 : h * LAT + (c + 1) * 128]
                    .reshape(PAD, 128)
                    .astype(f32)
                )
            qr = (
                msg_r[j, :, :, HL * LAT + h * ROT : HL * LAT + (h + 1) * ROT]
                .reshape(PAD, ROT)
                .astype(f32)
            )
            A2[at : at + PAD, 0:ROT] = rotate(qr).astype(bf16).astype(f32)
            A2[at : at + PAD, ROT:] = jnp.zeros((PAD, 128 - ROT), f32)
    for s in range(SEQ):
        self_score = jnp.zeros((16, 128), f32)
        for c in range(LAT // 128):
            part = A.at[c][pl.ds(s, 16, stride=PAD), :]
            Q[s, :, c * 128 : (c + 1) * 128] = part.astype(bf16)
            self_score = self_score + part * nl32[s : s + 1, c * 128 : (c + 1) * 128]
        part = A2[pl.ds(s, 16, stride=PAD), :]
        Qr[s] = part.astype(bf16)
        total = jnp.sum(self_score, axis=-1, keepdims=True) + jnp.sum(
            part[:, 0:ROT] * nr32[s : s + 1, :], axis=-1, keepdims=True
        )
        ps_ref[s] = jnp.broadcast_to(total * scale, (16, 128))
    c_rope.wait()
    for c in (c_wo, c_wg, c_wu, c_wd):
        c.start()
    for g in range(3):
        group = range(4 * g, 4 * g + 4)
        with jax.named_scope(f"attend{g}"):
            for s in group:
                val = mm(Q[s], turned[s]) + mm(Qr[s, :, 0:ROT], rope[s])
                valid = lax.broadcasted_iota(jnp.int32, (16, LEN), 1) < lens[s]
                S[s] = jnp.where(valid, val * scale, -jnp.inf)
            for s in group:
                sc = S[s]
                own = ps_ref[s][:, 0:1]
                highest = jnp.maximum(jnp.max(sc, axis=-1, keepdims=True), own)
                e = jnp.exp(sc - highest)
                eo = jnp.exp(own - highest)
                total = jnp.sum(e, axis=-1, keepdims=True) + eo
                Pb[s] = (e / total).astype(bf16)
                ps_ref[s] = jnp.broadcast_to((eo / total).astype(bf16).astype(f32), (16, 128))
            for s in group:
                val = mm(Pb[s], cache[s]) + ps_ref[s][:, 0:1] * nl32[s : s + 1, :]
                for c in range(LAT // 128):
                    O.at[c][pl.ds(g * 64 + s % 4, 16, stride=4), :] = val[:, c * 128 : (c + 1) * 128]
            for c in range(LAT // 128):
                hl_s[g, :, :, :, c * 128 : (c + 1) * 128] = (
                    O[c, g * 64 : (g + 1) * 64, :].astype(bf16).reshape(TP, HL, 4, 128)
                )
        for d in (2, 1, 3):
            j = (t + d) % TP
            pltpu.make_async_remote_copy(
                src_ref=hl_s.at[g, j],
                dst_ref=hl_r.at[g, t],
                send_sem=hss,
                recv_sem=hrs,
                device_id={"tp": j},
                device_id_type=MESH,
            ).start()
        hl_r[g, t] = hl_s[g, t]
    c_wo.wait()
    with jax.named_scope("wait_tp2"):
        arrived(hl_r.at[:, 0:3], hrs)
        arrived(hl_s.at[:, 0:3], hss)
    vals = jnp.concatenate(
        [mm(hl_r[:, :, h].reshape(TP * PAD, LAT), wvh[h]).astype(bf16) for h in range(HL)], axis=1
    )
    p_s[...] = mm(vals, wo[...]).astype(bf16).reshape(3, TP, 4, D)
    ph3 = tp_copies(3, lambda j: p_s.at[:, j], p_r.at[t])
    for c in ph3:
        c.start()
    p_r[t] = p_s[:, t]
    with jax.named_scope("wait_tp3"):
        for c in ph3:
            c.wait()
    attn = p_r[0].reshape(PAD, D).astype(f32)
    for j in range(1, TP):
        attn = attn + p_r[j].reshape(PAD, D).astype(f32)
    attn = attn.astype(bf16).astype(f32)
    mixed = (tok32[...] + rms(attn, g_post[...].astype(f32))).astype(bf16).astype(f32)
    mixed_ref[...] = mixed
    gbuf[t] = rms(mixed, g_ffn[...].astype(f32)).astype(bf16).reshape(3, 4, D)
    ph4 = tp_copies(4, lambda j: gbuf.at[t], gbuf.at[t])
    for c in ph4:
        c.start()
    for c in (c_wg, c_wu, c_wd):
        c.wait()
    with jax.named_scope("wait_tp4"):
        for c in ph4:
            c.wait()

    group_rows = gbuf[...].reshape(TP * PAD, D)
    for k in range(4):
        n = EP // 4
        X[k * n : (k + 1) * n] = (
            mm(Dm[k * n * CAPP : (k + 1) * n * CAPP, :], group_rows)
            .astype(bf16)
            .reshape(n, CAPP, D)
        )
        for p in range(k * n, (k + 1) * n):
            if order[p]:
                pltpu.make_async_remote_copy(
                    src_ref=X.at[p],
                    dst_ref=R.at[p],
                    send_sem=dss,
                    recv_sem=drs.at[p // CHUNK],
                    device_id={"ep": ep_shift(me, order[p], 1)},
                    device_id_type=MESH,
                ).start()
            else:
                R[p] = X[p]

    for k in range(EP // CHUNK):
        lo, hi = k * CHUNK, (k + 1) * CHUNK
        with jax.named_scope(f"wait_dispatch{k}"):
            arrived(R.at[lo : min(hi, EP - 1)], drs.at[k])
        flat = R[lo:hi].reshape(CHUNK * CAPP, D)
        gate = jnp.minimum(mm(flat, wg[...]), clamp_limit)
        upward = jnp.clip(mm(flat, wu[...]), -clamp_limit, clamp_limit)
        active = ((upward + 1.0) * gate * jax.nn.sigmoid(sigmoid_alpha * gate)).astype(bf16)
        Y[lo:hi] = mm(active, wd[...]).astype(bf16).reshape(CHUNK, CAPP, D)
        for p in range(lo, hi):
            d = order[p]
            if d:
                pltpu.make_async_remote_copy(
                    src_ref=Y.at[p],
                    dst_ref=T.at[p],
                    send_sem=ess,
                    recv_sem=ers,
                    device_id={"ep": ep_shift(me, d, -1)},
                    device_id_type=MESH,
                ).start()
            else:
                T[p] = Y[p]
    with jax.named_scope("wait_return"):
        arrived(T.at[0 : EP - 1], ers)
    both = mm(Cm[...], T[...].reshape(EP * CAPP, D))
    m_s[...] = (both[0 : TP * PAD] + both[TP * PAD :]).astype(bf16).reshape(TP, 3, 4, D)
    ph5 = tp_copies(5, lambda j: m_s.at[j], m_r.at[t])
    for c in ph5:
        c.start()
    m_r[t] = m_s[t]
    with jax.named_scope("wait_tp5"):
        for c in ph5:
            c.wait()
    with jax.named_scope("final"):
      moe = m_r[0].reshape(PAD, D).astype(f32)
      for j in range(1, TP):
        moe = moe + m_r[j].reshape(PAD, D).astype(f32)
      moe = moe.astype(bf16).astype(f32)
      arrived(X.at[0 : EP - 1], dss)
      arrived(Y.at[0 : EP - 1], ess)
      res = (mixed_ref[...] + rms(moe, g_post2[...].astype(f32))).astype(bf16)
      out_ref[...] = res


def finish_kernel(a, b, c, x, y, z, sem):
    copies = [pltpu.make_async_copy(p, q, sem.at[i]) for i, (p, q) in enumerate(((a, x), (b, y), (c, z)))]
    for p in copies:
        p.start()
    for p in copies:
        p.wait()


def body(
    tokens,
    cache_latent,
    cache_rope,
    lengths,
    attn_gain,
    latent_gain,
    post_attn_gain,
    ffn_gain,
    post_ffn_gain,
    w_query,
    w_query_rot,
    w_latent,
    w_key_rot,
    w_key_up,
    w_value_up,
    w_out,
    route_logits,
    routes,
    w_gate,
    w_up,
    w_down,
):
    vm = pl.BlockSpec(memory_space=pltpu.VMEM)
    hbm = pl.BlockSpec(memory_space=pl.ANY)
    V = pltpu.VMEM
    scratch = [
        pltpu.SMEM((SEQ,), jnp.int32),
        V((SEQ, D), bf16),
        V((4, TP * SEQ), jnp.int32),
        V((4, TP * SEQ), f32),
        V((D,), bf16),
        V((LAT,), bf16),
        V((D,), bf16),
        V((D,), bf16),
        V((D,), bf16),
        V((PAD, D), f32),
        V((TP, 3, 4, D), bf16),
        V((D, 512), bf16),
        V((D, 256), bf16),
        V((D, 128), bf16),
        V((ROT, D), bf16),
        V((HL * LAT, 128), bf16),
        V((HL * LAT, 128), bf16),
        V((2, HL * LAT, 128), f32),
        V((HL, LAT, 128), bf16),
        V((HL, LAT, 128), bf16),
        V((TP, 3, 4, MSG), bf16),
        V((TP, 3, 4, MSG), bf16),
        V((SEQ, LEN, LAT), bf16),
        V((SEQ, LAT, LEN), bf16),
        V((SEQ, ROT, LEN), bf16),
        V((LAT // 128, 16 * PAD, 128), f32),
        V((16 * PAD, 128), f32),
        V((SEQ, 16, LAT), bf16),
        V((SEQ, 16, 128), bf16),
        V((SEQ, 16, LEN), f32),
        V((SEQ, 16, LEN), bf16),
        V((SEQ, 16, 128), f32),
        V((LAT // 128, 16 * PAD, 128), f32),
        V((3, TP, HL, 4, LAT), bf16),
        V((3, TP, HL, 4, LAT), bf16),
        V((512, D), bf16),
        V((3, TP, 4, D), bf16),
        V((TP, 3, 4, D), bf16),
        V((TP, 3, 4, D), bf16),
        V((PAD, D), f32),
        V((EP * CAPP, TP * PAD), bf16),
        V((2 * TP * PAD, EP * CAPP), bf16),
        V((EP, CAPP, D), bf16),
        V((EP, CAPP, D), bf16),
        V((EP, CAPP, D), bf16),
        V((EP, CAPP, D), bf16),
        V((D, 512), bf16),
        V((D, 512), bf16),
        V((512, D), bf16),
        V((TP, 3, 4, D), bf16),
        V((TP, 3, 4, D), bf16),
        pltpu.SemaphoreType.DMA((19,)),
        pltpu.SemaphoreType.DMA((SEQ,)),
        pltpu.SemaphoreType.DMA,
        pltpu.SemaphoreType.DMA((6, 4)),
        pltpu.SemaphoreType.DMA((6, 4)),
        pltpu.SemaphoreType.DMA,
        pltpu.SemaphoreType.DMA,
        pltpu.SemaphoreType.DMA,
        pltpu.SemaphoreType.DMA((EP // CHUNK,)),
        pltpu.SemaphoreType.DMA,
        pltpu.SemaphoreType.DMA,
    ]
    parts = pl.pallas_call(
        layer_kernel,
        name="layer",
        out_shape=(
            pltpu.VMEM((SEQ, D), bf16),
            pltpu.VMEM((SEQ, LAT), bf16),
            pltpu.VMEM((SEQ, ROT), bf16),
        ),
        in_specs=[hbm] * 21,
        out_specs=(vm, vm, vm),
        scratch_shapes=scratch,
        compiler_params=pltpu.CompilerParams(
            collective_id=0, has_side_effects=True, vmem_limit_bytes=60 * 1024 * 1024
        ),
    )(
        lengths,
        tokens,
        routes.T,
        route_logits.T,
        attn_gain,
        latent_gain,
        post_attn_gain,
        ffn_gain,
        post_ffn_gain,
        cache_latent,
        cache_rope,
        w_query,
        w_query_rot,
        w_latent,
        w_key_rot.T,
        w_key_up.reshape(-1, w_key_up.shape[2]),
        w_value_up.reshape(-1, w_value_up.shape[2]),
        w_out,
        w_gate,
        w_up,
        w_down,
    )
    parts = [pltpu.with_memory_space_constraint(p, pltpu.VMEM) for p in parts]
    return pl.pallas_call(
        finish_kernel,
        name="finish",
        out_shape=(
            jax.ShapeDtypeStruct((SEQ, D), bf16),
            jax.ShapeDtypeStruct((SEQ, LAT), bf16),
            jax.ShapeDtypeStruct((SEQ, ROT), bf16),
        ),
        in_specs=[vm] * 3,
        out_specs=(hbm,) * 3,
        scratch_shapes=[pltpu.SemaphoreType.DMA((3,))],
    )(*parts)


def solution(mesh):
    return jax.shard_map(
        body,
        mesh=mesh,
        in_specs=(
            P(("ep", "tp"), None),
            P(("ep", "tp"), None, None),
            P(("ep", "tp"), None, None),
            P(("ep", "tp")),
            P(),
            P(),
            P(),
            P(),
            P(),
            P(None, "tp"),
            P(None, "tp"),
            P(None, "tp"),
            P(),
            P(None, "tp", None),
            P(None, "tp", None),
            P("tp", None),
            P("ep", None),
            P("ep", None),
            P("ep", None, "tp"),
            P("ep", None, "tp"),
            P("ep", "tp", None),
        ),
        out_specs=(P(("ep", "tp"), None), P(("ep", "tp"), None), P(("ep", "tp"), None)),
        check_vma=False,
    )
```

```python
import functools
import math

import jax
import jax.numpy as jnp
from jax import lax
from jax.experimental import pallas as pl
from jax.experimental.pallas import tpu as pltpu
from jax.sharding import PartitionSpec as P

MESH = pl.DeviceIdType.MESH
eps_norm = 1e-06
clamp_limit = 7.0
sigmoid_alpha = 1.702
theta_base = 10000.0
f32 = jnp.float32
bf16 = jnp.bfloat16

SEQ = 12
PAD = 12
D = 2048
LAT = 512
ROT = 64
LEN = 1024
HL = 4
TP = 4
EP = 32
CAPP = 8
MSG = HL * LAT + HL * ROT + 128


def hops(a):
    return min(a, 4 - a)


far_first = sorted(range(1, EP), key=lambda d: -(hops(d // 8) + hops((d // 2) % 4)))


order = far_first[::-1] + [0]
CHUNK = 16
QB = 128
DA = D - TP * QB


def ep_shift(me, d, sign):
    z, y, c = me // 8, (me // 2) % 4, me % 2
    dz, dy, dc = d // 8, (d // 2) % 4, d % 2
    if sign < 0:
        dz, dy = (4 - dz) % 4, (4 - dy) % 4
    return ((z + dz) % 4) * 8 + ((y + dy) % 4) * 2 + (c + dc) % 2


def mm(a, b):
    return lax.dot_general(a, b, (((1,), (0,)), ((), ())), preferred_element_type=f32)


def mm_nt(a, b):
    return lax.dot_general(a, b, (((1,), (1,)), ((), ())), preferred_element_type=f32)


def rms(v, gain):
    mean_square = jnp.mean(v * v, axis=-1, keepdims=True)
    return v * lax.rsqrt(mean_square + eps_norm) * gain


def layer_kernel(
    h_lens,
    h_tok,
    h_routes,
    h_logits,
    h_attn,
    h_lat,
    h_post,
    h_ffn,
    h_post2,
    h_clat,
    h_crope,
    h_wq,
    h_wqr,
    h_wl,
    h_wkr,
    h_wku,
    h_wvu,
    h_wo,
    h_wg,
    h_wu,
    h_wd,
    out_ref,
    lat_ref,
    rope_ref,
    lens,
    tok_in,
    routes_in,
    logits_in,
    g_attn,
    g_lat,
    g_post,
    g_ffn,
    g_post2,
    tok32,
    nbuf,
    wq,
    wqr,
    wl,
    wkr,
    wku,
    wvu,
    wtmp,
    wkh,
    wvh,
    msg_s,
    msg_r,
    cache,
    turned,
    rope,
    A,
    A2,
    Q,
    Qr,
    S,
    Pb,
    ps_ref,
    O,
    hl_s,
    hl_r,
    wo,
    p_s,
    p_r,
    ffn_own,
    g_quarter,
    g_rest,
    mixed_ref,
    Dm,
    Cm,
    X,
    R,
    Y,
    T,
    wg,
    wu,
    wd,
    m_s,
    m_r,
    lsem,
    csem,
    rsem,
    tss,
    trs,
    hss,
    hrs,
    YB,
    SB,
    dss,
    drs,
    ess,
    ers,
    dsb,
    drb,
    xgs,
    xgr,
    ybs,
    ybr,
    sbs,
    sbr,
):
    me = lax.axis_index("ep")
    t = lax.axis_index("tp")
    barrier = pltpu.get_barrier_semaphore()
    for d in (1, 2, 3):
        pl.semaphore_signal(barrier, inc=1, device_id={"tp": (t + d) % TP}, device_id_type=MESH)
    for d in far_first:
        pl.semaphore_signal(barrier, inc=1, device_id={"ep": ep_shift(me, d, 1)}, device_id_type=MESH)

    def local(src, dst, i):
        return pltpu.make_async_copy(src, dst, lsem.at[i])

    c_wq = local(h_wq, wq, 0)
    c_wqr = local(h_wqr, wqr, 1)
    c_wl = local(h_wl, wl, 2)
    c_wkr = local(h_wkr, wkr, 3)
    c_wku = local(h_wku, wku, 4)
    c_wvu = local(h_wvu, wvu, 5)
    c_wo = local(h_wo, wo, 6)
    c_wg = local(h_wg.at[0], wg, 7)
    c_wu = local(h_wu.at[0], wu, 8)
    c_wd = local(h_wd.at[0], wd, 9)
    c_tok = local(h_tok, tok_in, 10)
    c_attn = local(h_attn, g_attn, 11)
    c_lens = local(h_lens, lens, 12)
    c_routes = local(h_routes, routes_in, 13)
    c_logits = local(h_logits, logits_in, 14)
    c_lat = local(h_lat, g_lat, 15)
    c_post = local(h_post, g_post, 16)
    c_ffn = local(h_ffn, g_ffn, 17)
    c_post2 = local(h_post2, g_post2, 18)
    small = (c_lens, c_routes, c_logits, c_lat, c_post, c_ffn, c_post2)
    for c in (c_tok, c_attn) + small + (c_wku, c_wvu, c_wq, c_wqr, c_wl, c_wkr):
        c.start()

    def cache_copy(s):
        return pltpu.make_async_copy(h_clat.at[s], cache.at[s], csem.at[s])

    c_rope = pltpu.make_async_copy(h_crope, rope, rsem)

    c_rope.start()
    for s in range(SEQ):
        cache_copy(s).start()

    def arrived(ref, sem):
        pltpu.make_async_copy(ref, ref, sem).wait()

    def tp_wait(phase, src, dst):
        arrived(dst, trs.at[phase])
        arrived(src, tss.at[phase])

    def turn(s):
        cache_copy(s).wait()
        turned[s] = cache[s].T

    def tp_copies(phase, src, dst):
        out = []
        for d in (2, 1, 3):
            j = (t + d) % TP
            out.append(
                pltpu.make_async_remote_copy(
                    src_ref=src(j),
                    dst_ref=dst,
                    send_sem=tss.at[phase],
                    recv_sem=trs.at[phase],
                    device_id={"tp": j},
                    device_id_type=MESH,
                )
            )
        return out

    c_tok.wait()
    c_attn.wait()
    tok32[...] = tok_in[...].astype(f32)
    normed = rms(tok32[...], g_attn[...].astype(f32)).astype(bf16)
    nbuf[t] = normed.reshape(3, 4, D)
    with jax.named_scope("wait_barrier"):
        pl.semaphore_wait(barrier, 34)
    ph0 = tp_copies(0, lambda j: nbuf.at[t], nbuf.at[t])
    for c in ph0:
        c.start()

    for c in small:
        c.wait()

    logits = logits_in[...]
    raised = jnp.exp(logits - jnp.max(logits, axis=0, keepdims=True))
    rw = raised / jnp.sum(raised, axis=0, keepdims=True)
    ids = routes_in[...]
    place = lax.broadcasted_iota(jnp.int32, (EP, TP * PAD), 0)
    expert_of = jnp.zeros((EP, TP * PAD), jnp.int32)
    for p, d in enumerate(order):
        expert_of = jnp.where(place == p, ep_shift(me, d, 1), expert_of)
    member = jnp.zeros((EP, TP * PAD), f32)
    weight = jnp.zeros((EP, TP * PAD), f32)
    for k in range(4):
        hit = ids[k : k + 1, :] == expert_of
        member = member + jnp.where(hit, 1.0, 0.0)
        weight = weight + jnp.where(hit, rw[k : k + 1, :], 0.0)
    earlier = (
        lax.broadcasted_iota(jnp.int32, (TP * PAD, TP * PAD), 0)
        < lax.broadcasted_iota(jnp.int32, (TP * PAD, TP * PAD), 1)
    )
    member_b = member.astype(bf16)
    rank = mm(member_b, jnp.where(earlier, 1.0, 0.0).astype(bf16))
    spread = jnp.where(
        lax.broadcasted_iota(jnp.int32, (EP * CAPP, EP), 0) // CAPP
        == lax.broadcasted_iota(jnp.int32, (EP * CAPP, EP), 1),
        1.0,
        0.0,
    ).astype(bf16)
    slot = (lax.broadcasted_iota(jnp.int32, (EP * CAPP, TP * PAD), 0) % CAPP).astype(f32)
    dm = jnp.where(
        (mm(spread, member_b) > 0.5) & (mm(spread, rank.astype(bf16)) == slot), 1.0, 0.0
    )
    Dm[...] = dm.astype(bf16)
    w_hi = weight.astype(bf16)
    w_lo = (weight - w_hi.astype(f32)).astype(bf16)
    Cm[0 : TP * PAD, :] = jnp.transpose(mm(spread, w_hi) * dm).astype(bf16)
    Cm[TP * PAD :, :] = jnp.transpose(mm(spread, w_lo) * dm).astype(bf16)

    row = lax.broadcasted_iota(jnp.int32, (PAD, ROT), 0)
    col = lax.broadcasted_iota(jnp.int32, (PAD, ROT), 1)
    pos = jnp.zeros((PAD, ROT), f32)
    for s in range(SEQ):
        pos = jnp.where(row == s, lens[s].astype(f32), pos)
    half = ROT // 2
    freq = jnp.exp((col % half).astype(f32) * (-math.log(theta_base) / half))
    angle = pos * freq
    cosine = jnp.cos(angle)
    sine = jnp.where(col < half, -jnp.sin(angle), jnp.sin(angle))

    def rotate(v):
        swapped = jnp.concatenate([v[:, half:], v[:, :half]], axis=1)
        return v * cosine + swapped * sine

    with jax.named_scope("wait_up"):
        c_wku.wait()
        c_wvu.wait()
    wtmp[0] = wku[...].astype(f32)
    wtmp[1] = wvu[...].astype(f32)
    for h in range(HL):
        wkh[h] = wtmp.at[0][pl.ds(h, LAT, stride=HL), :].astype(bf16)
        wvh[h] = wtmp.at[1][pl.ds(h, LAT, stride=HL), :].astype(bf16)

    c_wkr.wait()
    key_raw = mm_nt(normed, wkr[...]).astype(bf16)
    new_rope = rotate(key_raw.astype(f32)).astype(bf16)
    rope_ref[...] = new_rope
    with jax.named_scope("turn0"):
        for s in range(4):
            turn(s)
    with jax.named_scope("wait_wq"):
        c_wq.wait()
        c_wqr.wait()
        c_wl.wait()
    with jax.named_scope("wait_tp0"):
        tp_wait(0, nbuf.at[0:3], nbuf.at[0:3])

    rows = nbuf[...].reshape(TP * PAD, D)
    qp = mm(rows, wq[...]).astype(bf16)
    cut = 2 * LAT
    for part in range(2):
        for h in (2 * part, 2 * part + 1):
            ql = mm_nt(qp[:, h * 128 : (h + 1) * 128], wkh[h]).astype(bf16)
            msg_s[:, :, :, h * LAT : (h + 1) * LAT] = ql.reshape(TP, 3, 4, LAT)
        if part:
            msg_s[:, :, :, HL * LAT : HL * LAT + HL * ROT] = (
                mm(rows, wqr[...]).astype(bf16).reshape(TP, 3, 4, HL * ROT)
            )
            msg_s[:, :, :, HL * LAT + HL * ROT :] = (
                mm(rows, wl[...]).astype(bf16).reshape(TP, 3, 4, 128)
            )
        cols = pl.ds(cut, MSG - cut) if part else pl.ds(0, cut)
        for c in tp_copies(
            1 + part, lambda j: msg_s.at[j, :, :, cols], msg_r.at[t, :, :, cols]
        ):
            c.start()
    msg_r[t] = msg_s[t]
    with jax.named_scope("turn1"):
        for s in range(4, SEQ):
            turn(s)
    with jax.named_scope("wait_tp1"):
        tp_wait(1, msg_s.at[0:3, :, :, 0:cut], msg_r.at[0:3, :, :, 0:cut])
        tp_wait(2, msg_s.at[0:3, :, :, cut:], msg_r.at[0:3, :, :, cut:])

    lat_raw = jnp.concatenate([msg_r[j, :, :, MSG - 128 :].reshape(PAD, 128) for j in range(TP)], axis=1)
    new_latent = rms(lat_raw.astype(f32), g_lat[...].astype(f32)).astype(bf16)
    lat_ref[...] = new_latent
    nl32 = new_latent.astype(f32)
    nr32 = new_rope.astype(f32)
    scale = (128 + ROT) ** (-0.5)
    for j in range(TP):
        for h in range(HL):
            at = (j * HL + h) * PAD
            for c in range(LAT // 128):
                A[c, at : at + PAD, :] = (
                    msg_r[j, :, :, h * LAT + c * 128 : h * LAT + (c + 1) * 128]
                    .reshape(PAD, 128)
                    .astype(f32)
                )
            qr = (
                msg_r[j, :, :, HL * LAT + h * ROT : HL * LAT + (h + 1) * ROT]
                .reshape(PAD, ROT)
                .astype(f32)
            )
            A2[at : at + PAD, 0:ROT] = rotate(qr).astype(bf16).astype(f32)
            A2[at : at + PAD, ROT:] = jnp.zeros((PAD, 128 - ROT), f32)
    for s in range(SEQ):
        self_score = jnp.zeros((16, 128), f32)
        for c in range(LAT // 128):
            part = A.at[c][pl.ds(s, 16, stride=PAD), :]
            Q[s, :, c * 128 : (c + 1) * 128] = part.astype(bf16)
            self_score = self_score + part * nl32[s : s + 1, c * 128 : (c + 1) * 128]
        part = A2[pl.ds(s, 16, stride=PAD), :]
        Qr[s] = part.astype(bf16)
        total = jnp.sum(self_score, axis=-1, keepdims=True) + jnp.sum(
            part[:, 0:ROT] * nr32[s : s + 1, :], axis=-1, keepdims=True
        )
        ps_ref[s] = jnp.broadcast_to(total * scale, (16, 128))
    c_rope.wait()
    for c in (c_wo, c_wg, c_wu, c_wd):
        c.start()
    for g in range(3):
        group = range(4 * g, 4 * g + 4)
        with jax.named_scope(f"attend{g}"):
            for s in group:
                val = mm(Q[s], turned[s]) + mm(Qr[s, :, 0:ROT], rope[s])
                valid = lax.broadcasted_iota(jnp.int32, (16, LEN), 1) < lens[s]
                S[s] = jnp.where(valid, val * scale, -jnp.inf)
            for s in group:
                sc = S[s]
                own = ps_ref[s][:, 0:1]
                highest = jnp.maximum(jnp.max(sc, axis=-1, keepdims=True), own)
                e = jnp.exp(sc - highest)
                eo = jnp.exp(own - highest)
                total = jnp.sum(e, axis=-1, keepdims=True) + eo
                Pb[s] = (e * (1.0 / total)).astype(bf16)
                ps_ref[s] = jnp.broadcast_to((eo / total).astype(bf16).astype(f32), (16, 128))
            for s in group:
                val = mm(Pb[s], cache[s]) + ps_ref[s][:, 0:1] * nl32[s : s + 1, :]
                for c in range(LAT // 128):
                    O.at[c][pl.ds(g * 64 + s % 4, 16, stride=4), :] = val[:, c * 128 : (c + 1) * 128]
            for c in range(LAT // 128):
                hl_s[g, :, :, :, c * 128 : (c + 1) * 128] = (
                    O[c, g * 64 : (g + 1) * 64, :].astype(bf16).reshape(TP, HL, 4, 128)
                )
        for d in (2, 1, 3):
            j = (t + d) % TP
            pltpu.make_async_remote_copy(
                src_ref=hl_s.at[g, j],
                dst_ref=hl_r.at[g, t],
                send_sem=hss,
                recv_sem=hrs,
                device_id={"tp": j},
                device_id_type=MESH,
            ).start()
        hl_r[g, t] = hl_s[g, t]
    c_wo.wait()
    with jax.named_scope("wait_tp2"):
        arrived(hl_r.at[:, 0:3], hrs)
        arrived(hl_s.at[:, 0:3], hss)
    vals = jnp.concatenate(
        [mm(hl_r[:, :, h].reshape(TP * PAD, LAT), wvh[h]).astype(bf16) for h in range(HL)], axis=1
    )
    p_s[...] = mm(vals, wo[...]).astype(bf16).reshape(3, TP, 4, D)
    ph3 = tp_copies(3, lambda j: p_s.at[:, j], p_r.at[t])
    for c in ph3:
        c.start()
    p_r[t] = p_s[:, t]
    with jax.named_scope("wait_tp3"):
        tp_wait(3, p_s.at[:, 0:3], p_r.at[0:3])
    attn = p_r[0].reshape(PAD, D).astype(f32)
    for j in range(1, TP):
        attn = attn + p_r[j].reshape(PAD, D).astype(f32)
    attn = attn.astype(bf16).astype(f32)
    mixed = (tok32[...] + rms(attn, g_post[...].astype(f32))).astype(bf16).astype(f32)
    mixed_ref[...] = mixed
    ffn = rms(mixed, g_ffn[...].astype(f32)).astype(bf16)
    ffn_own[...] = ffn.reshape(3, 4, D)
    mine = pl.ds(pl.multiple_of(DA + QB * t, 128), QB)
    rest = pl.ds(0, DA)
    for c in tp_copies(
        4, lambda j: ffn_own.at[:, :, pl.ds(pl.multiple_of(DA + QB * j, 128), QB)], g_quarter.at[t]
    ):
        c.start()
    for c in tp_copies(6, lambda j: ffn_own.at[:, :, rest], g_rest.at[t]):
        c.start()
    g_quarter[t] = ffn_own[:, :, mine]
    g_rest[t] = ffn_own[:, :, rest]
    for c in (c_wg, c_wu, c_wd):
        c.wait()
    with jax.named_scope("wait_tp4"):
        tp_wait(4, g_quarter.at[0:3], g_quarter.at[0:3])
    def ep_send(src, dst, ssem, rsem, shift):
        pltpu.make_async_remote_copy(
            src_ref=src,
            dst_ref=dst,
            send_sem=ssem,
            recv_sem=rsem,
            device_id={"ep": shift},
            device_id_type=MESH,
        ).start()

    X[:, :, mine] = (
        mm(Dm[...], g_quarter[...].reshape(TP * PAD, QB)).astype(bf16).reshape(EP, CAPP, QB)
    )
    for p in range(EP - 1):
        to = ep_shift(me, order[p], 1)
        ep_send(X.at[p, :, mine], R.at[p, :, mine], dsb, drb.at[p // CHUNK], to)
    R[EP - 1, :, mine] = X[EP - 1, :, mine]
    with jax.named_scope("wait_tp6"):
        tp_wait(6, g_rest.at[0:3], g_rest.at[0:3])
    rows_rest = g_rest[...].reshape(TP * PAD, DA)
    for k in range(4):
        n = EP // 4
        X[k * n : (k + 1) * n, :, rest] = (
            mm(Dm[k * n * CAPP : (k + 1) * n * CAPP, :], rows_rest)
            .astype(bf16)
            .reshape(n, CAPP, DA)
        )
        for p in range(k * n, min((k + 1) * n, EP - 1)):
            to = ep_shift(me, order[p], 1)
            ep_send(X.at[p, :, rest], R.at[p, :, rest], dss, drs.at[p // CHUNK], to)
    R[EP - 1, :, rest] = X[EP - 1, :, rest]
    chunks = [(k, k * CHUNK, (k + 1) * CHUNK, min((k + 1) * CHUNK, EP - 1)) for k in range(EP // CHUNK)]
    for k, lo, hi, last in chunks:
        with jax.named_scope(f"wait_quarter{k}"):
            arrived(R.at[lo:last, :, mine], drb.at[k])
        for d in (2, 1, 3):
            pltpu.make_async_remote_copy(
                src_ref=R.at[lo:hi, :, mine],
                dst_ref=R.at[lo:hi, :, mine],
                send_sem=xgs.at[k],
                recv_sem=xgr.at[k],
                device_id={"tp": (t + d) % TP},
                device_id_type=MESH,
            ).start()

    for k, lo, hi, last in chunks:
        with jax.named_scope(f"wait_dispatch{k}"):
            arrived(R.at[lo:last, :, rest], drs.at[k])
        with jax.named_scope(f"wait_gather{k}"):
            arrived(R.at[lo:hi, :, 0 : 3 * QB], xgr.at[k])
        flat = R[lo:hi].reshape(CHUNK * CAPP, D)
        gate = jnp.minimum(mm(flat, wg[...]), clamp_limit)
        upward = jnp.clip(mm(flat, wu[...]), -clamp_limit, clamp_limit)
        active = ((upward + 1.0) * gate * jax.nn.sigmoid(sigmoid_alpha * gate)).astype(bf16)
        Y[lo:hi] = mm(active, wd[...]).astype(bf16).reshape(CHUNK, CAPP, D)
        for d in (2, 1, 3):
            j = (t + d) % TP
            pltpu.make_async_remote_copy(
                src_ref=Y.at[lo:hi, :, pl.ds(pl.multiple_of(DA + QB * j, 128), QB)],
                dst_ref=YB.at[t, lo:hi],
                send_sem=ybs.at[k],
                recv_sem=ybr.at[k],
                device_id={"tp": j},
                device_id_type=MESH,
            ).start()
        for p in range(lo, last):
            to = ep_shift(me, order[p], -1)
            ep_send(Y.at[p, :, rest], T.at[p, :, rest], ess, ers, to)
        YB[t, lo:hi] = Y[lo:hi, :, mine]
    T[EP - 1, :, rest] = Y[EP - 1, :, rest]
    for k, lo, hi, last in chunks:
        with jax.named_scope(f"wait_sum{k}"):
            arrived(YB.at[0:3, lo:hi], ybr.at[k])
        summed = YB[0, lo:hi].astype(f32)
        for j in range(1, TP):
            summed = summed + YB[j, lo:hi].astype(f32)
        SB[lo:hi] = summed.astype(bf16)
        for p in range(lo, last):
            to = ep_shift(me, order[p], -1)
            ep_send(SB.at[p], T.at[p, :, mine], sbs, sbr, to)
    T[EP - 1, :, mine] = SB[EP - 1]
    with jax.named_scope("wait_return"):
        arrived(T.at[0 : EP - 1, :, rest], ers)
    with jax.named_scope("wait_return_sum"):
        arrived(SB.at[0 : EP - 1], sbr)
    for at, wide, cols in ((0, DA, rest), (DA, QB, mine)):
        both = mm(Cm[...], T[:, :, cols].reshape(EP * CAPP, wide))
        m_s[:, :, :, at : at + wide] = (
            (both[0 : TP * PAD] + both[TP * PAD :]).astype(bf16).reshape(TP, 3, 4, wide)
        )
    ph5 = tp_copies(5, lambda j: m_s.at[j], m_r.at[t])
    for c in ph5:
        c.start()
    m_r[t] = m_s[t]
    with jax.named_scope("wait_tp5"):
        tp_wait(5, m_s.at[0:3], m_r.at[0:3])
    arrived(X.at[0 : EP - 1, :, rest], dss)
    arrived(X.at[0 : EP - 1, :, mine], dsb)
    arrived(Y.at[0 : EP - 1, :, rest], ess)
    arrived(SB.at[0 : EP - 1], sbs)
    for k, lo, hi, last in chunks:
        arrived(R.at[lo:hi, :, 0 : 3 * QB], xgs.at[k])
        arrived(YB.at[0:3, lo:hi], ybs.at[k])
    with jax.named_scope("final"):
      moe = m_r[0, :, :, 0:DA].reshape(PAD, DA).astype(f32)
      for j in range(1, TP):
        moe = moe + m_r[j, :, :, 0:DA].reshape(PAD, DA).astype(f32)
      parts = [m_r[j, :, :, DA:].reshape(PAD, QB).astype(f32) for j in range(TP)]
      moe = jnp.concatenate([moe] + parts, axis=1)
      moe = moe.astype(bf16).astype(f32)
      res = (mixed_ref[...] + rms(moe, g_post2[...].astype(f32))).astype(bf16)
      out_ref[...] = res


def finish_kernel(a, b, c, x, y, z, sem):
    copies = [pltpu.make_async_copy(p, q, sem.at[i]) for i, (p, q) in enumerate(((a, x), (b, y), (c, z)))]
    for p in copies:
        p.start()
    for p in copies:
        p.wait()


def body(
    tokens,
    cache_latent,
    cache_rope,
    lengths,
    attn_gain,
    latent_gain,
    post_attn_gain,
    ffn_gain,
    post_ffn_gain,
    w_query,
    w_query_rot,
    w_latent,
    w_key_rot,
    w_key_up,
    w_value_up,
    w_out,
    route_logits,
    routes,
    w_gate,
    w_up,
    w_down,
):
    vm = pl.BlockSpec(memory_space=pltpu.VMEM)
    hbm = pl.BlockSpec(memory_space=pl.ANY)
    V = pltpu.VMEM
    scratch = [
        pltpu.SMEM((SEQ,), jnp.int32),
        V((SEQ, D), bf16),
        V((4, TP * SEQ), jnp.int32),
        V((4, TP * SEQ), f32),
        V((D,), bf16),
        V((LAT,), bf16),
        V((D,), bf16),
        V((D,), bf16),
        V((D,), bf16),
        V((PAD, D), f32),
        V((TP, 3, 4, D), bf16),
        V((D, 512), bf16),
        V((D, 256), bf16),
        V((D, 128), bf16),
        V((ROT, D), bf16),
        V((HL * LAT, 128), bf16),
        V((HL * LAT, 128), bf16),
        V((2, HL * LAT, 128), f32),
        V((HL, LAT, 128), bf16),
        V((HL, LAT, 128), bf16),
        V((TP, 3, 4, MSG), bf16),
        V((TP, 3, 4, MSG), bf16),
        V((SEQ, LEN, LAT), bf16),
        V((SEQ, LAT, LEN), bf16),
        V((SEQ, ROT, LEN), bf16),
        V((LAT // 128, 16 * PAD, 128), f32),
        V((16 * PAD, 128), f32),
        V((SEQ, 16, LAT), bf16),
        V((SEQ, 16, 128), bf16),
        V((SEQ, 16, LEN), f32),
        V((SEQ, 16, LEN), bf16),
        V((SEQ, 16, 128), f32),
        V((LAT // 128, 16 * PAD, 128), f32),
        V((3, TP, HL, 4, LAT), bf16),
        V((3, TP, HL, 4, LAT), bf16),
        V((512, D), bf16),
        V((3, TP, 4, D), bf16),
        V((TP, 3, 4, D), bf16),
        V((3, 4, D), bf16),
        V((TP, 3, 4, QB), bf16),
        V((TP, 3, 4, DA), bf16),
        V((PAD, D), f32),
        V((EP * CAPP, TP * PAD), bf16),
        V((2 * TP * PAD, EP * CAPP), bf16),
        V((EP, CAPP, D), bf16),
        V((EP, CAPP, D), bf16),
        V((EP, CAPP, D), bf16),
        V((EP, CAPP, D), bf16),
        V((D, 512), bf16),
        V((D, 512), bf16),
        V((512, D), bf16),
        V((TP, 3, 4, DA + QB), bf16),
        V((TP, 3, 4, DA + QB), bf16),
        pltpu.SemaphoreType.DMA((19,)),
        pltpu.SemaphoreType.DMA((SEQ,)),
        pltpu.SemaphoreType.DMA,
        pltpu.SemaphoreType.DMA((7,)),
        pltpu.SemaphoreType.DMA((7,)),
        pltpu.SemaphoreType.DMA,
        pltpu.SemaphoreType.DMA,
        V((TP, EP, CAPP, QB), bf16),
        V((EP, CAPP, QB), bf16),
        pltpu.SemaphoreType.DMA,
        pltpu.SemaphoreType.DMA((EP // CHUNK,)),
        pltpu.SemaphoreType.DMA,
        pltpu.SemaphoreType.DMA,
        pltpu.SemaphoreType.DMA,
        pltpu.SemaphoreType.DMA((EP // CHUNK,)),
        pltpu.SemaphoreType.DMA((EP // CHUNK,)),
        pltpu.SemaphoreType.DMA((EP // CHUNK,)),
        pltpu.SemaphoreType.DMA((EP // CHUNK,)),
        pltpu.SemaphoreType.DMA((EP // CHUNK,)),
        pltpu.SemaphoreType.DMA,
        pltpu.SemaphoreType.DMA,
    ]
    parts = pl.pallas_call(
        layer_kernel,
        name="layer",
        out_shape=(
            pltpu.VMEM((SEQ, D), bf16),
            pltpu.VMEM((SEQ, LAT), bf16),
            pltpu.VMEM((SEQ, ROT), bf16),
        ),
        in_specs=[hbm] * 21,
        out_specs=(vm, vm, vm),
        scratch_shapes=scratch,
        compiler_params=pltpu.CompilerParams(
            collective_id=0, has_side_effects=True, vmem_limit_bytes=60 * 1024 * 1024
        ),
    )(
        lengths,
        tokens,
        routes.T,
        route_logits.T,
        attn_gain,
        latent_gain,
        post_attn_gain,
        ffn_gain,
        post_ffn_gain,
        cache_latent,
        cache_rope,
        w_query,
        w_query_rot,
        w_latent,
        w_key_rot.T,
        w_key_up.reshape(-1, w_key_up.shape[2]),
        w_value_up.reshape(-1, w_value_up.shape[2]),
        w_out,
        w_gate,
        w_up,
        w_down,
    )
    parts = [pltpu.with_memory_space_constraint(p, pltpu.VMEM) for p in parts]
    return pl.pallas_call(
        finish_kernel,
        name="finish",
        out_shape=(
            jax.ShapeDtypeStruct((SEQ, D), bf16),
            jax.ShapeDtypeStruct((SEQ, LAT), bf16),
            jax.ShapeDtypeStruct((SEQ, ROT), bf16),
        ),
        in_specs=[vm] * 3,
        out_specs=(hbm,) * 3,
        scratch_shapes=[pltpu.SemaphoreType.DMA((3,))],
    )(*parts)


def solution(mesh):
    return jax.shard_map(
        body,
        mesh=mesh,
        in_specs=(
            P(("ep", "tp"), None),
            P(("ep", "tp"), None, None),
            P(("ep", "tp"), None, None),
            P(("ep", "tp")),
            P(),
            P(),
            P(),
            P(),
            P(),
            P(None, "tp"),
            P(None, "tp"),
            P(None, "tp"),
            P(),
            P(None, "tp", None),
            P(None, "tp", None),
            P("tp", None),
            P("ep", None),
            P("ep", None),
            P("ep", None, "tp"),
            P("ep", None, "tp"),
            P("ep", "tp", None),
        ),
        out_specs=(P(("ep", "tp"), None), P(("ep", "tp"), None), P(("ep", "tp"), None)),
        check_vma=False,
    )
```

```python
import functools
import math

import jax
import jax.numpy as jnp
from jax import lax
from jax.experimental import pallas as pl
from jax.experimental.pallas import tpu as pltpu
from jax.sharding import PartitionSpec as P

MESH = pl.DeviceIdType.MESH
eps_norm = 1e-06
clamp_limit = 7.0
sigmoid_alpha = 1.702
theta_base = 10000.0
f32 = jnp.float32
bf16 = jnp.bfloat16

SEQ = 12
PAD = 12
D = 2048
LAT = 512
ROT = 64
LEN = 1024
HL = 4
TP = 4
EP = 32
CAPP = 8
MSG = HL * LAT + HL * ROT + 128


def hops(a):
    return min(a, 4 - a)


far_first = sorted(range(1, EP), key=lambda d: -(hops(d // 8) + hops((d // 2) % 4)))


order = far_first[::-1] + [0]
CHUNK = 8
QB = 128
DA = D - TP * QB
QR = 256
DR = D - TP * QR


def ep_shift(me, d, sign):
    z, y, c = me // 8, (me // 2) % 4, me % 2
    dz, dy, dc = d // 8, (d // 2) % 4, d % 2
    if sign < 0:
        dz, dy = (4 - dz) % 4, (4 - dy) % 4
    return ((z + dz) % 4) * 8 + ((y + dy) % 4) * 2 + (c + dc) % 2


def mm(a, b):
    return lax.dot_general(a, b, (((1,), (0,)), ((), ())), preferred_element_type=f32)


def mm_nt(a, b):
    return lax.dot_general(a, b, (((1,), (1,)), ((), ())), preferred_element_type=f32)


def rms(v, gain):
    mean_square = jnp.mean(v * v, axis=-1, keepdims=True)
    return v * lax.rsqrt(mean_square + eps_norm) * gain


def layer_kernel(
    h_lens,
    h_tok,
    h_routes,
    h_logits,
    h_attn,
    h_lat,
    h_post,
    h_ffn,
    h_post2,
    h_clat,
    h_crope,
    h_wq,
    h_wqr,
    h_wl,
    h_wkr,
    h_wku,
    h_wvu,
    h_wo,
    h_wg,
    h_wu,
    h_wd,
    out_ref,
    lat_ref,
    rope_ref,
    lens,
    tok_in,
    routes_in,
    logits_in,
    g_attn,
    g_lat,
    g_post,
    g_ffn,
    g_post2,
    tok32,
    nbuf,
    wq,
    wqr,
    wl,
    wkr,
    wku,
    wvu,
    wtmp,
    wkh,
    wvh,
    msg_s,
    msg_r,
    cache,
    turned,
    rope,
    A,
    A2,
    Q,
    Qr,
    S,
    Pb,
    ps_ref,
    O,
    hl_s,
    hl_r,
    wo,
    p_s,
    p_r,
    ffn_own,
    g_quarter,
    g_rest,
    mixed_ref,
    Dm,
    Cm,
    X,
    R,
    Y,
    T,
    wg,
    wu,
    wd,
    m_s,
    m_r,
    lsem,
    csem,
    rsem,
    tss,
    trs,
    hss,
    hrs,
    YB,
    SB,
    dss,
    drs,
    ess,
    ers,
    dsb,
    drb,
    xgs,
    xgr,
    ybs,
    ybr,
    sbs,
    sbr,
):
    me = lax.axis_index("ep")
    t = lax.axis_index("tp")
    barrier = pltpu.get_barrier_semaphore()
    for d in (1, 2, 3):
        pl.semaphore_signal(barrier, inc=1, device_id={"tp": (t + d) % TP}, device_id_type=MESH)
    for d in far_first:
        pl.semaphore_signal(barrier, inc=1, device_id={"ep": ep_shift(me, d, 1)}, device_id_type=MESH)

    def local(src, dst, i):
        return pltpu.make_async_copy(src, dst, lsem.at[i])

    c_wq = local(h_wq, wq, 0)
    c_wqr = local(h_wqr, wqr, 1)
    c_wl = local(h_wl, wl, 2)
    c_wkr = local(h_wkr, wkr, 3)
    c_wku = local(h_wku, wku, 4)
    c_wvu = local(h_wvu, wvu, 5)
    c_wo = local(h_wo, wo, 6)
    c_wg = local(h_wg.at[0], wg, 7)
    c_wu = local(h_wu.at[0], wu, 8)
    c_wd = local(h_wd.at[0], wd, 9)
    c_tok = local(h_tok, tok_in, 10)
    c_attn = local(h_attn, g_attn, 11)
    c_lens = local(h_lens, lens, 12)
    c_routes = local(h_routes, routes_in, 13)
    c_logits = local(h_logits, logits_in, 14)
    c_lat = local(h_lat, g_lat, 15)
    c_post = local(h_post, g_post, 16)
    c_ffn = local(h_ffn, g_ffn, 17)
    c_post2 = local(h_post2, g_post2, 18)
    small = (c_lens, c_routes, c_logits, c_lat, c_post, c_ffn, c_post2)
    for c in (c_tok, c_attn) + small + (c_wku, c_wvu):
        c.start()

    def cache_copy(s):
        return pltpu.make_async_copy(h_clat.at[s], cache.at[s], csem.at[s])

    c_rope = pltpu.make_async_copy(h_crope, rope, rsem)

    def fetch(g):
        for s in range(4 * g, 4 * g + 4):
            cache_copy(s).start()

    fetch(0)

    def arrived(ref, sem):
        pltpu.make_async_copy(ref, ref, sem).wait()

    def tp_wait(phase, src, dst):
        arrived(dst, trs.at[phase])
        arrived(src, tss.at[phase])

    def turn(s):
        cache_copy(s).wait()
        turned[s] = cache[s].T

    def tp_copies(phase, src, dst):
        out = []
        for d in (2, 1, 3):
            j = (t + d) % TP
            out.append(
                pltpu.make_async_remote_copy(
                    src_ref=src(j),
                    dst_ref=dst,
                    send_sem=tss.at[phase],
                    recv_sem=trs.at[phase],
                    device_id={"tp": j},
                    device_id_type=MESH,
                )
            )
        return out

    c_tok.wait()
    c_attn.wait()
    tok32[...] = tok_in[...].astype(f32)
    normed = rms(tok32[...], g_attn[...].astype(f32)).astype(bf16)
    nbuf[t] = normed.reshape(3, 4, D)
    with jax.named_scope("wait_barrier"):
        pl.semaphore_wait(barrier, 34)
    ph0 = tp_copies(0, lambda j: nbuf.at[t], nbuf.at[t])
    for c in ph0 + [c_wq, c_wqr, c_wl, c_wkr]:
        c.start()

    for c in small:
        c.wait()

    logits = logits_in[...]
    raised = jnp.exp(logits - jnp.max(logits, axis=0, keepdims=True))
    rw = raised / jnp.sum(raised, axis=0, keepdims=True)
    ids = routes_in[...]
    place = lax.broadcasted_iota(jnp.int32, (EP, TP * PAD), 0)
    expert_of = jnp.zeros((EP, TP * PAD), jnp.int32)
    for p, d in enumerate(order):
        expert_of = jnp.where(place == p, ep_shift(me, d, 1), expert_of)
    member = jnp.zeros((EP, TP * PAD), f32)
    weight = jnp.zeros((EP, TP * PAD), f32)
    for k in range(4):
        hit = ids[k : k + 1, :] == expert_of
        member = member + jnp.where(hit, 1.0, 0.0)
        weight = weight + jnp.where(hit, rw[k : k + 1, :], 0.0)
    earlier = (
        lax.broadcasted_iota(jnp.int32, (TP * PAD, TP * PAD), 0)
        < lax.broadcasted_iota(jnp.int32, (TP * PAD, TP * PAD), 1)
    )
    member_b = member.astype(bf16)
    rank = mm(member_b, jnp.where(earlier, 1.0, 0.0).astype(bf16))
    spread = jnp.where(
        lax.broadcasted_iota(jnp.int32, (EP * CAPP, EP), 0) // CAPP
        == lax.broadcasted_iota(jnp.int32, (EP * CAPP, EP), 1),
        1.0,
        0.0,
    ).astype(bf16)
    slot = (lax.broadcasted_iota(jnp.int32, (EP * CAPP, TP * PAD), 0) % CAPP).astype(f32)
    dm = jnp.where(
        (mm(spread, member_b) > 0.5) & (mm(spread, rank.astype(bf16)) == slot), 1.0, 0.0
    )
    Dm[...] = dm.astype(bf16)
    w_hi = weight.astype(bf16)
    w_lo = (weight - w_hi.astype(f32)).astype(bf16)
    Cm[0 : TP * PAD, :] = jnp.transpose(mm(spread, w_hi) * dm).astype(bf16)
    Cm[TP * PAD :, :] = jnp.transpose(mm(spread, w_lo) * dm).astype(bf16)

    row = lax.broadcasted_iota(jnp.int32, (PAD, ROT), 0)
    col = lax.broadcasted_iota(jnp.int32, (PAD, ROT), 1)
    pos = jnp.zeros((PAD, ROT), f32)
    for s in range(SEQ):
        pos = jnp.where(row == s, lens[s].astype(f32), pos)
    half = ROT // 2
    freq = jnp.exp((col % half).astype(f32) * (-math.log(theta_base) / half))
    angle = pos * freq
    cosine = jnp.cos(angle)
    sine = jnp.where(col < half, -jnp.sin(angle), jnp.sin(angle))

    def rotate(v):
        swapped = jnp.concatenate([v[:, half:], v[:, :half]], axis=1)
        return v * cosine + swapped * sine

    with jax.named_scope("wait_up"):
        c_wku.wait()
        c_wvu.wait()
    wtmp[0] = wku[...].astype(f32)
    wtmp[1] = wvu[...].astype(f32)
    for h in range(HL):
        wkh[h] = wtmp.at[0][pl.ds(h, LAT, stride=HL), :].astype(bf16)
        wvh[h] = wtmp.at[1][pl.ds(h, LAT, stride=HL), :].astype(bf16)

    with jax.named_scope("turn0"):
        for s in range(4):
            turn(s)
    c_rope.start()
    fetch(1)
    with jax.named_scope("wait_wq"):
        c_wq.wait()
        c_wqr.wait()
        c_wl.wait()
    with jax.named_scope("wait_tp0"):
        tp_wait(0, nbuf.at[0:3], nbuf.at[0:3])

    fetch(2)
    rows = nbuf[...].reshape(TP * PAD, D)
    qp = mm(rows, wq[...]).astype(bf16)
    cut = 2 * LAT
    for part in range(2):
        for h in (2 * part, 2 * part + 1):
            ql = mm_nt(qp[:, h * 128 : (h + 1) * 128], wkh[h]).astype(bf16)
            msg_s[:, :, :, h * LAT : (h + 1) * LAT] = ql.reshape(TP, 3, 4, LAT)
        if part:
            msg_s[:, :, :, HL * LAT : HL * LAT + HL * ROT] = (
                mm(rows, wqr[...]).astype(bf16).reshape(TP, 3, 4, HL * ROT)
            )
            msg_s[:, :, :, HL * LAT + HL * ROT :] = (
                mm(rows, wl[...]).astype(bf16).reshape(TP, 3, 4, 128)
            )
        cols = pl.ds(cut, MSG - cut) if part else pl.ds(0, cut)
        for c in tp_copies(
            1 + part, lambda j: msg_s.at[j, :, :, cols], msg_r.at[t, :, :, cols]
        ):
            c.start()
    msg_r[t] = msg_s[t]
    c_wkr.wait()
    key_raw = mm_nt(normed, wkr[...]).astype(bf16)
    new_rope = rotate(key_raw.astype(f32)).astype(bf16)
    rope_ref[...] = new_rope
    with jax.named_scope("turn1"):
        for s in range(4, SEQ):
            turn(s)
    with jax.named_scope("wait_tp1"):
        tp_wait(1, msg_s.at[0:3, :, :, 0:cut], msg_r.at[0:3, :, :, 0:cut])
        tp_wait(2, msg_s.at[0:3, :, :, cut:], msg_r.at[0:3, :, :, cut:])

    lat_raw = jnp.concatenate([msg_r[j, :, :, MSG - 128 :].reshape(PAD, 128) for j in range(TP)], axis=1)
    new_latent = rms(lat_raw.astype(f32), g_lat[...].astype(f32)).astype(bf16)
    lat_ref[...] = new_latent
    nl32 = new_latent.astype(f32)
    nr32 = new_rope.astype(f32)
    scale = (128 + ROT) ** (-0.5)
    for j in range(TP):
        for h in range(HL):
            at = (j * HL + h) * PAD
            for c in range(LAT // 128):
                A[c, at : at + PAD, :] = (
                    msg_r[j, :, :, h * LAT + c * 128 : h * LAT + (c + 1) * 128]
                    .reshape(PAD, 128)
                    .astype(f32)
                )
            qr = (
                msg_r[j, :, :, HL * LAT + h * ROT : HL * LAT + (h + 1) * ROT]
                .reshape(PAD, ROT)
                .astype(f32)
            )
            A2[at : at + PAD, 0:ROT] = rotate(qr).astype(bf16).astype(f32)
            A2[at : at + PAD, ROT:] = jnp.zeros((PAD, 128 - ROT), f32)
    for s in range(SEQ):
        self_score = jnp.zeros((16, 128), f32)
        for c in range(LAT // 128):
            part = A.at[c][pl.ds(s, 16, stride=PAD), :]
            Q[s, :, c * 128 : (c + 1) * 128] = part.astype(bf16)
            self_score = self_score + part * nl32[s : s + 1, c * 128 : (c + 1) * 128]
        part = A2[pl.ds(s, 16, stride=PAD), :]
        Qr[s] = part.astype(bf16)
        total = jnp.sum(self_score, axis=-1, keepdims=True) + jnp.sum(
            part[:, 0:ROT] * nr32[s : s + 1, :], axis=-1, keepdims=True
        )
        ps_ref[s] = jnp.broadcast_to(total * scale, (16, 128))
    c_rope.wait()
    for c in (c_wo, c_wg, c_wu, c_wd):
        c.start()
    for g in range(3):
        group = range(4 * g, 4 * g + 4)
        with jax.named_scope(f"attend{g}"):
            for s in group:
                val = mm(Q[s], turned[s]) + mm(Qr[s, :, 0:ROT], rope[s])
                valid = lax.broadcasted_iota(jnp.int32, (16, LEN), 1) < lens[s]
                S[s] = jnp.where(valid, val * scale, -jnp.inf)
            for s in group:
                sc = S[s]
                own = ps_ref[s][:, 0:1]
                highest = jnp.maximum(jnp.max(sc, axis=-1, keepdims=True), own)
                e = jnp.exp(sc - highest)
                eo = jnp.exp(own - highest)
                total = jnp.sum(e, axis=-1, keepdims=True) + eo
                Pb[s] = (e * (1.0 / total)).astype(bf16)
                ps_ref[s] = jnp.broadcast_to((eo / total).astype(bf16).astype(f32), (16, 128))
            for s in group:
                val = mm(Pb[s], cache[s]) + ps_ref[s][:, 0:1] * nl32[s : s + 1, :]
                for c in range(LAT // 128):
                    O.at[c][pl.ds(g * 64 + s % 4, 16, stride=4), :] = val[:, c * 128 : (c + 1) * 128]
            for c in range(LAT // 128):
                hl_s[g, :, :, :, c * 128 : (c + 1) * 128] = (
                    O[c, g * 64 : (g + 1) * 64, :].astype(bf16).reshape(TP, HL, 4, 128)
                )
        for d in (2, 1, 3):
            j = (t + d) % TP
            pltpu.make_async_remote_copy(
                src_ref=hl_s.at[g, j],
                dst_ref=hl_r.at[g, t],
                send_sem=hss,
                recv_sem=hrs,
                device_id={"tp": j},
                device_id_type=MESH,
            ).start()
        hl_r[g, t] = hl_s[g, t]
    c_wo.wait()
    with jax.named_scope("wait_tp2"):
        arrived(hl_r.at[:, 0:3], hrs)
        arrived(hl_s.at[:, 0:3], hss)
    vals = jnp.concatenate(
        [mm(hl_r[:, :, h].reshape(TP * PAD, LAT), wvh[h]).astype(bf16) for h in range(HL)], axis=1
    )
    p_s[...] = mm(vals, wo[...]).astype(bf16).reshape(3, TP, 4, D)
    ph3 = tp_copies(3, lambda j: p_s.at[:, j], p_r.at[t])
    for c in ph3:
        c.start()
    p_r[t] = p_s[:, t]
    with jax.named_scope("wait_tp3"):
        tp_wait(3, p_s.at[:, 0:3], p_r.at[0:3])
    attn = p_r[0].reshape(PAD, D).astype(f32)
    for j in range(1, TP):
        attn = attn + p_r[j].reshape(PAD, D).astype(f32)
    attn = attn.astype(bf16).astype(f32)
    mixed = (tok32[...] + rms(attn, g_post[...].astype(f32))).astype(bf16).astype(f32)
    mixed_ref[...] = mixed
    ffn = rms(mixed, g_ffn[...].astype(f32)).astype(bf16)
    ffn_own[...] = ffn.reshape(3, 4, D)
    mine = pl.ds(pl.multiple_of(DA + QB * t, 128), QB)
    rest = pl.ds(0, DA)
    mine_r = pl.ds(pl.multiple_of(DR + QR * t, 128), QR)
    rest_r = pl.ds(0, DR)
    for c in tp_copies(
        4, lambda j: ffn_own.at[:, :, pl.ds(pl.multiple_of(DA + QB * j, 128), QB)], g_quarter.at[t]
    ):
        c.start()
    for c in tp_copies(6, lambda j: ffn_own.at[:, :, rest], g_rest.at[t]):
        c.start()
    g_quarter[t] = ffn_own[:, :, mine]
    g_rest[t] = ffn_own[:, :, rest]
    for c in (c_wg, c_wu, c_wd):
        c.wait()
    with jax.named_scope("wait_tp4"):
        tp_wait(4, g_quarter.at[0:3], g_quarter.at[0:3])
    def ep_send(src, dst, ssem, rsem, shift):
        pltpu.make_async_remote_copy(
            src_ref=src,
            dst_ref=dst,
            send_sem=ssem,
            recv_sem=rsem,
            device_id={"ep": shift},
            device_id_type=MESH,
        ).start()

    X[:, :, mine] = (
        mm(Dm[...], g_quarter[...].reshape(TP * PAD, QB)).astype(bf16).reshape(EP, CAPP, QB)
    )
    for p in range(EP - 1):
        to = ep_shift(me, order[p], 1)
        ep_send(X.at[p, :, mine], R.at[p, :, mine], dsb, drb.at[p // CHUNK], to)
    R[EP - 1, :, mine] = X[EP - 1, :, mine]
    with jax.named_scope("wait_tp6"):
        tp_wait(6, g_rest.at[0:3], g_rest.at[0:3])
    rows_rest = g_rest[...].reshape(TP * PAD, DA)
    for k in range(4):
        n = EP // 4
        X[k * n : (k + 1) * n, :, rest] = (
            mm(Dm[k * n * CAPP : (k + 1) * n * CAPP, :], rows_rest)
            .astype(bf16)
            .reshape(n, CAPP, DA)
        )
        for p in range(k * n, min((k + 1) * n, EP - 1)):
            to = ep_shift(me, order[p], 1)
            ep_send(X.at[p, :, rest], R.at[p, :, rest], dss, drs.at[p // CHUNK], to)
    R[EP - 1, :, rest] = X[EP - 1, :, rest]
    chunks = [(k, k * CHUNK, (k + 1) * CHUNK, min((k + 1) * CHUNK, EP - 1)) for k in range(EP // CHUNK)]
    for k, lo, hi, last in chunks:
        with jax.named_scope(f"wait_quarter{k}"):
            arrived(R.at[lo:last, :, mine], drb.at[k])
        for d in (2, 1, 3):
            pltpu.make_async_remote_copy(
                src_ref=R.at[lo:hi, :, mine],
                dst_ref=R.at[lo:hi, :, mine],
                send_sem=xgs.at[k],
                recv_sem=xgr.at[k],
                device_id={"tp": (t + d) % TP},
                device_id_type=MESH,
            ).start()

    for k, lo, hi, last in chunks:
        with jax.named_scope(f"wait_dispatch{k}"):
            arrived(R.at[lo:last, :, rest], drs.at[k])
        with jax.named_scope(f"wait_gather{k}"):
            arrived(R.at[lo:hi, :, 0 : 3 * QB], xgr.at[k])
        flat = R[lo:hi].reshape(CHUNK * CAPP, D)
        gate = jnp.minimum(mm(flat, wg[...]), clamp_limit)
        upward = jnp.clip(mm(flat, wu[...]), -clamp_limit, clamp_limit)
        active = ((upward + 1.0) * gate * jax.nn.sigmoid(sigmoid_alpha * gate)).astype(bf16)
        Y[lo:hi] = mm(active, wd[...]).astype(bf16).reshape(CHUNK, CAPP, D)
        for d in (2, 1, 3):
            j = (t + d) % TP
            pltpu.make_async_remote_copy(
                src_ref=Y.at[lo:hi, :, pl.ds(pl.multiple_of(DR + QR * j, 128), QR)],
                dst_ref=YB.at[t, lo:hi],
                send_sem=ybs.at[k],
                recv_sem=ybr.at[k],
                device_id={"tp": j},
                device_id_type=MESH,
            ).start()
        for p in range(lo, last):
            to = ep_shift(me, order[p], -1)
            ep_send(Y.at[p, :, rest_r], T.at[p, :, rest_r], ess, ers, to)
        YB[t, lo:hi] = Y[lo:hi, :, mine_r]
    T[EP - 1, :, rest_r] = Y[EP - 1, :, rest_r]
    for k, lo, hi, last in chunks:
        with jax.named_scope(f"wait_sum{k}"):
            arrived(YB.at[0:3, lo:hi], ybr.at[k])
        summed = YB[0, lo:hi].astype(f32)
        for j in range(1, TP):
            summed = summed + YB[j, lo:hi].astype(f32)
        SB[lo:hi] = summed.astype(bf16)
        for p in range(lo, last):
            to = ep_shift(me, order[p], -1)
            ep_send(SB.at[p], T.at[p, :, mine_r], sbs, sbr, to)
    T[EP - 1, :, mine_r] = SB[EP - 1]
    with jax.named_scope("wait_return"):
        arrived(T.at[0 : EP - 1, :, rest_r], ers)
    with jax.named_scope("wait_return_sum"):
        arrived(SB.at[0 : EP - 1], sbr)
    for at, wide, cols in ((0, DR, rest_r), (DR, QR, mine_r)):
        both = mm(Cm[...], T[:, :, cols].reshape(EP * CAPP, wide))
        m_s[:, :, :, at : at + wide] = (
            (both[0 : TP * PAD] + both[TP * PAD :]).astype(bf16).reshape(TP, 3, 4, wide)
        )
    ph5 = tp_copies(5, lambda j: m_s.at[j], m_r.at[t])
    for c in ph5:
        c.start()
    m_r[t] = m_s[t]
    with jax.named_scope("wait_tp5"):
        tp_wait(5, m_s.at[0:3], m_r.at[0:3])
    arrived(X.at[0 : EP - 1, :, rest], dss)
    arrived(X.at[0 : EP - 1, :, mine], dsb)
    arrived(Y.at[0 : EP - 1, :, rest_r], ess)
    arrived(SB.at[0 : EP - 1], sbs)
    for k, lo, hi, last in chunks:
        arrived(R.at[lo:hi, :, 0 : 3 * QB], xgs.at[k])
        arrived(YB.at[0:3, lo:hi], ybs.at[k])
    with jax.named_scope("final"):
      moe = m_r[0, :, :, 0:DR].reshape(PAD, DR).astype(f32)
      for j in range(1, TP):
        moe = moe + m_r[j, :, :, 0:DR].reshape(PAD, DR).astype(f32)
      parts = [m_r[j, :, :, DR:].reshape(PAD, QR).astype(f32) for j in range(TP)]
      moe = jnp.concatenate([moe] + parts, axis=1)
      moe = moe.astype(bf16).astype(f32)
      res = (mixed_ref[...] + rms(moe, g_post2[...].astype(f32))).astype(bf16)
      out_ref[...] = res


def finish_kernel(a, b, c, x, y, z, sem):
    copies = [pltpu.make_async_copy(p, q, sem.at[i]) for i, (p, q) in enumerate(((a, x), (b, y), (c, z)))]
    for p in copies:
        p.start()
    for p in copies:
        p.wait()


def body(
    tokens,
    cache_latent,
    cache_rope,
    lengths,
    attn_gain,
    latent_gain,
    post_attn_gain,
    ffn_gain,
    post_ffn_gain,
    w_query,
    w_query_rot,
    w_latent,
    w_key_rot,
    w_key_up,
    w_value_up,
    w_out,
    route_logits,
    routes,
    w_gate,
    w_up,
    w_down,
):
    vm = pl.BlockSpec(memory_space=pltpu.VMEM)
    hbm = pl.BlockSpec(memory_space=pl.ANY)
    V = pltpu.VMEM
    scratch = [
        pltpu.SMEM((SEQ,), jnp.int32),
        V((SEQ, D), bf16),
        V((4, TP * SEQ), jnp.int32),
        V((4, TP * SEQ), f32),
        V((D,), bf16),
        V((LAT,), bf16),
        V((D,), bf16),
        V((D,), bf16),
        V((D,), bf16),
        V((PAD, D), f32),
        V((TP, 3, 4, D), bf16),
        V((D, 512), bf16),
        V((D, 256), bf16),
        V((D, 128), bf16),
        V((ROT, D), bf16),
        V((HL * LAT, 128), bf16),
        V((HL * LAT, 128), bf16),
        V((2, HL * LAT, 128), f32),
        V((HL, LAT, 128), bf16),
        V((HL, LAT, 128), bf16),
        V((TP, 3, 4, MSG), bf16),
        V((TP, 3, 4, MSG), bf16),
        V((SEQ, LEN, LAT), bf16),
        V((SEQ, LAT, LEN), bf16),
        V((SEQ, ROT, LEN), bf16),
        V((LAT // 128, 16 * PAD, 128), f32),
        V((16 * PAD, 128), f32),
        V((SEQ, 16, LAT), bf16),
        V((SEQ, 16, 128), bf16),
        V((SEQ, 16, LEN), f32),
        V((SEQ, 16, LEN), bf16),
        V((SEQ, 16, 128), f32),
        V((LAT // 128, 16 * PAD, 128), f32),
        V((3, TP, HL, 4, LAT), bf16),
        V((3, TP, HL, 4, LAT), bf16),
        V((512, D), bf16),
        V((3, TP, 4, D), bf16),
        V((TP, 3, 4, D), bf16),
        V((3, 4, D), bf16),
        V((TP, 3, 4, QB), bf16),
        V((TP, 3, 4, DA), bf16),
        V((PAD, D), f32),
        V((EP * CAPP, TP * PAD), bf16),
        V((2 * TP * PAD, EP * CAPP), bf16),
        V((EP, CAPP, D), bf16),
        V((EP, CAPP, D), bf16),
        V((EP, CAPP, D), bf16),
        V((EP, CAPP, D), bf16),
        V((D, 512), bf16),
        V((D, 512), bf16),
        V((512, D), bf16),
        V((TP, 3, 4, DR + QR), bf16),
        V((TP, 3, 4, DR + QR), bf16),
        pltpu.SemaphoreType.DMA((19,)),
        pltpu.SemaphoreType.DMA((SEQ,)),
        pltpu.SemaphoreType.DMA,
        pltpu.SemaphoreType.DMA((7,)),
        pltpu.SemaphoreType.DMA((7,)),
        pltpu.SemaphoreType.DMA,
        pltpu.SemaphoreType.DMA,
        V((TP, EP, CAPP, QR), bf16),
        V((EP, CAPP, QR), bf16),
        pltpu.SemaphoreType.DMA,
        pltpu.SemaphoreType.DMA((EP // CHUNK,)),
        pltpu.SemaphoreType.DMA,
        pltpu.SemaphoreType.DMA,
        pltpu.SemaphoreType.DMA,
        pltpu.SemaphoreType.DMA((EP // CHUNK,)),
        pltpu.SemaphoreType.DMA((EP // CHUNK,)),
        pltpu.SemaphoreType.DMA((EP // CHUNK,)),
        pltpu.SemaphoreType.DMA((EP // CHUNK,)),
        pltpu.SemaphoreType.DMA((EP // CHUNK,)),
        pltpu.SemaphoreType.DMA,
        pltpu.SemaphoreType.DMA,
    ]
    parts = pl.pallas_call(
        layer_kernel,
        name="layer",
        out_shape=(
            pltpu.VMEM((SEQ, D), bf16),
            pltpu.VMEM((SEQ, LAT), bf16),
            pltpu.VMEM((SEQ, ROT), bf16),
        ),
        in_specs=[hbm] * 21,
        out_specs=(vm, vm, vm),
        scratch_shapes=scratch,
        compiler_params=pltpu.CompilerParams(
            collective_id=0, has_side_effects=True, vmem_limit_bytes=60 * 1024 * 1024
        ),
    )(
        lengths,
        tokens,
        routes.T,
        route_logits.T,
        attn_gain,
        latent_gain,
        post_attn_gain,
        ffn_gain,
        post_ffn_gain,
        cache_latent,
        cache_rope,
        w_query,
        w_query_rot,
        w_latent,
        w_key_rot.T,
        w_key_up.reshape(-1, w_key_up.shape[2]),
        w_value_up.reshape(-1, w_value_up.shape[2]),
        w_out,
        w_gate,
        w_up,
        w_down,
    )
    parts = [pltpu.with_memory_space_constraint(p, pltpu.VMEM) for p in parts]
    return pl.pallas_call(
        finish_kernel,
        name="finish",
        out_shape=(
            jax.ShapeDtypeStruct((SEQ, D), bf16),
            jax.ShapeDtypeStruct((SEQ, LAT), bf16),
            jax.ShapeDtypeStruct((SEQ, ROT), bf16),
        ),
        in_specs=[vm] * 3,
        out_specs=(hbm,) * 3,
        scratch_shapes=[pltpu.SemaphoreType.DMA((3,))],
    )(*parts)


def solution(mesh):
    return jax.shard_map(
        body,
        mesh=mesh,
        in_specs=(
            P(("ep", "tp"), None),
            P(("ep", "tp"), None, None),
            P(("ep", "tp"), None, None),
            P(("ep", "tp")),
            P(),
            P(),
            P(),
            P(),
            P(),
            P(None, "tp"),
            P(None, "tp"),
            P(None, "tp"),
            P(),
            P(None, "tp", None),
            P(None, "tp", None),
            P("tp", None),
            P("ep", None),
            P("ep", None),
            P("ep", None, "tp"),
            P("ep", None, "tp"),
            P("ep", "tp", None),
        ),
        out_specs=(P(("ep", "tp"), None), P(("ep", "tp"), None), P(("ep", "tp"), None)),
        check_vma=False,
    )
```

```python
import functools
import math

import jax
import jax.numpy as jnp
from jax import lax
from jax.experimental import pallas as pl
from jax.experimental.pallas import tpu as pltpu
from jax.sharding import PartitionSpec as P

MESH = pl.DeviceIdType.MESH
eps_norm = 1e-06
clamp_limit = 7.0
sigmoid_alpha = 1.702
theta_base = 10000.0
f32 = jnp.float32
bf16 = jnp.bfloat16

SEQ = 12
PAD = 12
D = 2048
LAT = 512
ROT = 64
LEN = 1024
HL = 4
TP = 4
EP = 32
CAPP = 8
MSG = HL * LAT + HL * ROT + 128


def hops(a):
    return min(a, 4 - a)


far_first = sorted(range(1, EP), key=lambda d: -(hops(d // 8) + hops((d // 2) % 4)))


order = far_first[::-1] + [0]
CHUNK = 8
LAG = 3
QB = 128
DA = D - TP * QB
QR = 256
DR = D - TP * QR


def ep_shift(me, d, sign):
    z, y, c = me // 8, (me // 2) % 4, me % 2
    dz, dy, dc = d // 8, (d // 2) % 4, d % 2
    if sign < 0:
        dz, dy = (4 - dz) % 4, (4 - dy) % 4
    return ((z + dz) % 4) * 8 + ((y + dy) % 4) * 2 + (c + dc) % 2


def mm(a, b):
    return lax.dot_general(a, b, (((1,), (0,)), ((), ())), preferred_element_type=f32)


def mm_nt(a, b):
    return lax.dot_general(a, b, (((1,), (1,)), ((), ())), preferred_element_type=f32)


def rms(v, gain):
    mean_square = jnp.mean(v * v, axis=-1, keepdims=True)
    return v * lax.rsqrt(mean_square + eps_norm) * gain


def layer_kernel(
    h_lens,
    h_tok,
    h_routes,
    h_logits,
    h_attn,
    h_lat,
    h_post,
    h_ffn,
    h_post2,
    h_clat,
    h_crope,
    h_wq,
    h_wqr,
    h_wl,
    h_wkr,
    h_wku,
    h_wvu,
    h_wo,
    h_wg,
    h_wu,
    h_wd,
    out_ref,
    lat_ref,
    rope_ref,
    lens,
    tok_in,
    routes_in,
    logits_in,
    g_attn,
    g_lat,
    g_post,
    g_ffn,
    g_post2,
    tok32,
    nbuf,
    wq,
    wqr,
    wl,
    wkr,
    wku,
    wvu,
    wtmp,
    wkh,
    wvh,
    msg_s,
    msg_r,
    cache,
    turned,
    rope,
    A,
    A2,
    Q,
    Qr,
    S,
    Pb,
    ps_ref,
    O,
    hl_s,
    hl_r,
    wo,
    p_s,
    p_r,
    ffn_own,
    g_quarter,
    g_rest,
    mixed_ref,
    Dm,
    Cm,
    X,
    R,
    Y,
    T,
    wg,
    wu,
    wd,
    m_s,
    m_r,
    lsem,
    csem,
    rsem,
    tss,
    trs,
    hss,
    hrs,
    YB,
    SB,
    dss,
    drs,
    ess,
    ers,
    dsb,
    drb,
    xgs,
    xgr,
    ybs,
    ybr,
    sbs,
    sbr,
):
    me = lax.axis_index("ep")
    t = lax.axis_index("tp")
    barrier = pltpu.get_barrier_semaphore()
    for d in (1, 2, 3):
        pl.semaphore_signal(barrier, inc=1, device_id={"tp": (t + d) % TP}, device_id_type=MESH)
    for d in far_first:
        pl.semaphore_signal(barrier, inc=1, device_id={"ep": ep_shift(me, d, 1)}, device_id_type=MESH)

    def local(src, dst, i):
        return pltpu.make_async_copy(src, dst, lsem.at[i])

    c_wq = local(h_wq, wq, 0)
    c_wqr = local(h_wqr, wqr, 1)
    c_wl = local(h_wl, wl, 2)
    c_wkr = local(h_wkr, wkr, 3)
    c_wku = local(h_wku, wku, 4)
    c_wvu = local(h_wvu, wvu, 5)
    c_wo = local(h_wo, wo, 6)
    c_wg = local(h_wg.at[0], wg, 7)
    c_wu = local(h_wu.at[0], wu, 8)
    c_wd = local(h_wd.at[0], wd, 9)
    c_tok = local(h_tok, tok_in, 10)
    c_attn = local(h_attn, g_attn, 11)
    c_lens = local(h_lens, lens, 12)
    c_routes = local(h_routes, routes_in, 13)
    c_logits = local(h_logits, logits_in, 14)
    c_lat = local(h_lat, g_lat, 15)
    c_post = local(h_post, g_post, 16)
    c_ffn = local(h_ffn, g_ffn, 17)
    c_post2 = local(h_post2, g_post2, 18)
    small = (c_lens, c_routes, c_logits, c_lat, c_post, c_ffn, c_post2)
    for c in (c_tok, c_attn) + small + (c_wku, c_wvu):
        c.start()

    def cache_copy(s):
        return pltpu.make_async_copy(h_clat.at[s], cache.at[s], csem.at[s])

    c_rope = pltpu.make_async_copy(h_crope, rope, rsem)

    def fetch(g):
        for s in range(4 * g, 4 * g + 4):
            cache_copy(s).start()

    fetch(0)

    def arrived(ref, sem):
        pltpu.make_async_copy(ref, ref, sem).wait()

    def tp_wait(phase, src, dst):
        arrived(dst, trs.at[phase])
        arrived(src, tss.at[phase])

    def turn(s):
        cache_copy(s).wait()
        turned[s] = cache[s].T

    def tp_copies(phase, src, dst):
        out = []
        for d in (2, 1, 3):
            j = (t + d) % TP
            out.append(
                pltpu.make_async_remote_copy(
                    src_ref=src(j),
                    dst_ref=dst,
                    send_sem=tss.at[phase],
                    recv_sem=trs.at[phase],
                    device_id={"tp": j},
                    device_id_type=MESH,
                )
            )
        return out

    c_tok.wait()
    c_attn.wait()
    tok32[...] = tok_in[...].astype(f32)
    normed = rms(tok32[...], g_attn[...].astype(f32)).astype(bf16)
    nbuf[t] = normed.reshape(3, 4, D)
    with jax.named_scope("wait_barrier"):
        pl.semaphore_wait(barrier, 34)
    ph0 = tp_copies(0, lambda j: nbuf.at[t], nbuf.at[t])
    for c in ph0 + [c_wq, c_wqr, c_wl, c_wkr]:
        c.start()

    for c in small:
        c.wait()

    logits = logits_in[...]
    raised = jnp.exp(logits - jnp.max(logits, axis=0, keepdims=True))
    rw = raised / jnp.sum(raised, axis=0, keepdims=True)
    ids = routes_in[...]
    place = lax.broadcasted_iota(jnp.int32, (EP, TP * PAD), 0)
    expert_of = jnp.zeros((EP, TP * PAD), jnp.int32)
    for p, d in enumerate(order):
        expert_of = jnp.where(place == p, ep_shift(me, d, 1), expert_of)
    member = jnp.zeros((EP, TP * PAD), f32)
    weight = jnp.zeros((EP, TP * PAD), f32)
    for k in range(4):
        hit = ids[k : k + 1, :] == expert_of
        member = member + jnp.where(hit, 1.0, 0.0)
        weight = weight + jnp.where(hit, rw[k : k + 1, :], 0.0)
    earlier = (
        lax.broadcasted_iota(jnp.int32, (TP * PAD, TP * PAD), 0)
        < lax.broadcasted_iota(jnp.int32, (TP * PAD, TP * PAD), 1)
    )
    member_b = member.astype(bf16)
    rank = mm(member_b, jnp.where(earlier, 1.0, 0.0).astype(bf16))
    spread = jnp.where(
        lax.broadcasted_iota(jnp.int32, (EP * CAPP, EP), 0) // CAPP
        == lax.broadcasted_iota(jnp.int32, (EP * CAPP, EP), 1),
        1.0,
        0.0,
    ).astype(bf16)
    slot = (lax.broadcasted_iota(jnp.int32, (EP * CAPP, TP * PAD), 0) % CAPP).astype(f32)
    dm = jnp.where(
        (mm(spread, member_b) > 0.5) & (mm(spread, rank.astype(bf16)) == slot), 1.0, 0.0
    )
    Dm[...] = dm.astype(bf16)
    w_hi = weight.astype(bf16)
    w_lo = (weight - w_hi.astype(f32)).astype(bf16)
    Cm[0 : TP * PAD, :] = jnp.transpose(mm(spread, w_hi) * dm).astype(bf16)
    Cm[TP * PAD :, :] = jnp.transpose(mm(spread, w_lo) * dm).astype(bf16)

    row = lax.broadcasted_iota(jnp.int32, (PAD, ROT), 0)
    col = lax.broadcasted_iota(jnp.int32, (PAD, ROT), 1)
    pos = jnp.zeros((PAD, ROT), f32)
    for s in range(SEQ):
        pos = jnp.where(row == s, lens[s].astype(f32), pos)
    half = ROT // 2
    freq = jnp.exp((col % half).astype(f32) * (-math.log(theta_base) / half))
    angle = pos * freq
    cosine = jnp.cos(angle)
    sine = jnp.where(col < half, -jnp.sin(angle), jnp.sin(angle))

    def rotate(v):
        swapped = jnp.concatenate([v[:, half:], v[:, :half]], axis=1)
        return v * cosine + swapped * sine

    with jax.named_scope("wait_up"):
        c_wku.wait()
        c_wvu.wait()
    wtmp[0] = wku[...].astype(f32)
    wtmp[1] = wvu[...].astype(f32)
    for h in range(HL):
        wkh[h] = wtmp.at[0][pl.ds(h, LAT, stride=HL), :].astype(bf16)
        wvh[h] = wtmp.at[1][pl.ds(h, LAT, stride=HL), :].astype(bf16)

    with jax.named_scope("turn0"):
        for s in range(4):
            turn(s)
    c_rope.start()
    fetch(1)
    with jax.named_scope("wait_wq"):
        c_wq.wait()
        c_wqr.wait()
        c_wl.wait()
    with jax.named_scope("wait_tp0"):
        tp_wait(0, nbuf.at[0:3], nbuf.at[0:3])

    fetch(2)
    rows = nbuf[...].reshape(TP * PAD, D)
    qp = mm(rows, wq[...]).astype(bf16)
    cut = 2 * LAT
    for part in range(2):
        for h in (2 * part, 2 * part + 1):
            ql = mm_nt(qp[:, h * 128 : (h + 1) * 128], wkh[h]).astype(bf16)
            msg_s[:, :, :, h * LAT : (h + 1) * LAT] = ql.reshape(TP, 3, 4, LAT)
        if part:
            msg_s[:, :, :, HL * LAT : HL * LAT + HL * ROT] = (
                mm(rows, wqr[...]).astype(bf16).reshape(TP, 3, 4, HL * ROT)
            )
            msg_s[:, :, :, HL * LAT + HL * ROT :] = (
                mm(rows, wl[...]).astype(bf16).reshape(TP, 3, 4, 128)
            )
        cols = pl.ds(cut, MSG - cut) if part else pl.ds(0, cut)
        for c in tp_copies(
            1 + part, lambda j: msg_s.at[j, :, :, cols], msg_r.at[t, :, :, cols]
        ):
            c.start()
    msg_r[t] = msg_s[t]
    c_wkr.wait()
    key_raw = mm_nt(normed, wkr[...]).astype(bf16)
    new_rope = rotate(key_raw.astype(f32)).astype(bf16)
    rope_ref[...] = new_rope
    with jax.named_scope("turn1"):
        for s in range(4, SEQ):
            turn(s)
    with jax.named_scope("wait_tp1"):
        tp_wait(1, msg_s.at[0:3, :, :, 0:cut], msg_r.at[0:3, :, :, 0:cut])
        tp_wait(2, msg_s.at[0:3, :, :, cut:], msg_r.at[0:3, :, :, cut:])

    lat_raw = jnp.concatenate([msg_r[j, :, :, MSG - 128 :].reshape(PAD, 128) for j in range(TP)], axis=1)
    new_latent = rms(lat_raw.astype(f32), g_lat[...].astype(f32)).astype(bf16)
    lat_ref[...] = new_latent
    nl32 = new_latent.astype(f32)
    nr32 = new_rope.astype(f32)
    scale = (128 + ROT) ** (-0.5)
    for j in range(TP):
        for h in range(HL):
            at = (j * HL + h) * PAD
            for c in range(LAT // 128):
                A[c, at : at + PAD, :] = (
                    msg_r[j, :, :, h * LAT + c * 128 : h * LAT + (c + 1) * 128]
                    .reshape(PAD, 128)
                    .astype(f32)
                )
            qr = (
                msg_r[j, :, :, HL * LAT + h * ROT : HL * LAT + (h + 1) * ROT]
                .reshape(PAD, ROT)
                .astype(f32)
            )
            A2[at : at + PAD, 0:ROT] = rotate(qr).astype(bf16).astype(f32)
            A2[at : at + PAD, ROT:] = jnp.zeros((PAD, 128 - ROT), f32)
    for s in range(SEQ):
        self_score = jnp.zeros((16, 128), f32)
        for c in range(LAT // 128):
            part = A.at[c][pl.ds(s, 16, stride=PAD), :]
            Q[s, :, c * 128 : (c + 1) * 128] = part.astype(bf16)
            self_score = self_score + part * nl32[s : s + 1, c * 128 : (c + 1) * 128]
        part = A2[pl.ds(s, 16, stride=PAD), :]
        Qr[s] = part.astype(bf16)
        total = jnp.sum(self_score, axis=-1, keepdims=True) + jnp.sum(
            part[:, 0:ROT] * nr32[s : s + 1, :], axis=-1, keepdims=True
        )
        ps_ref[s] = jnp.broadcast_to(total * scale, (16, 128))
    c_rope.wait()
    for c in (c_wo, c_wg, c_wu, c_wd):
        c.start()
    for g in range(3):
        group = range(4 * g, 4 * g + 4)
        with jax.named_scope(f"attend{g}"):
            for s in group:
                val = mm(Q[s], turned[s]) + mm(Qr[s, :, 0:ROT], rope[s])
                valid = lax.broadcasted_iota(jnp.int32, (16, LEN), 1) < lens[s]
                S[s] = jnp.where(valid, val * scale, -jnp.inf)
            for s in group:
                sc = S[s]
                own = ps_ref[s][:, 0:1]
                highest = jnp.maximum(jnp.max(sc, axis=-1, keepdims=True), own)
                e = jnp.exp(sc - highest)
                eo = jnp.exp(own - highest)
                total = jnp.sum(e, axis=-1, keepdims=True) + eo
                Pb[s] = (e * (1.0 / total)).astype(bf16)
                ps_ref[s] = jnp.broadcast_to((eo / total).astype(bf16).astype(f32), (16, 128))
            for s in group:
                val = mm(Pb[s], cache[s]) + ps_ref[s][:, 0:1] * nl32[s : s + 1, :]
                for c in range(LAT // 128):
                    O.at[c][pl.ds(g * 64 + s % 4, 16, stride=4), :] = val[:, c * 128 : (c + 1) * 128]
            for c in range(LAT // 128):
                hl_s[g, :, :, :, c * 128 : (c + 1) * 128] = (
                    O[c, g * 64 : (g + 1) * 64, :].astype(bf16).reshape(TP, HL, 4, 128)
                )
        for d in (2, 1, 3):
            j = (t + d) % TP
            pltpu.make_async_remote_copy(
                src_ref=hl_s.at[g, j],
                dst_ref=hl_r.at[g, t],
                send_sem=hss,
                recv_sem=hrs,
                device_id={"tp": j},
                device_id_type=MESH,
            ).start()
        hl_r[g, t] = hl_s[g, t]
    c_wo.wait()
    with jax.named_scope("wait_tp2"):
        arrived(hl_r.at[:, 0:3], hrs)
        arrived(hl_s.at[:, 0:3], hss)
    vals = jnp.concatenate(
        [mm(hl_r[:, :, h].reshape(TP * PAD, LAT), wvh[h]).astype(bf16) for h in range(HL)], axis=1
    )
    p_s[...] = mm(vals, wo[...]).astype(bf16).reshape(3, TP, 4, D)
    ph3 = tp_copies(3, lambda j: p_s.at[:, j], p_r.at[t])
    for c in ph3:
        c.start()
    p_r[t] = p_s[:, t]
    with jax.named_scope("wait_tp3"):
        tp_wait(3, p_s.at[:, 0:3], p_r.at[0:3])
    attn = p_r[0].reshape(PAD, D).astype(f32)
    for j in range(1, TP):
        attn = attn + p_r[j].reshape(PAD, D).astype(f32)
    attn = attn.astype(bf16).astype(f32)
    mixed = (tok32[...] + rms(attn, g_post[...].astype(f32))).astype(bf16).astype(f32)
    mixed_ref[...] = mixed
    ffn = rms(mixed, g_ffn[...].astype(f32)).astype(bf16)
    ffn_own[...] = ffn.reshape(3, 4, D)
    mine = pl.ds(pl.multiple_of(DA + QB * t, 128), QB)
    rest = pl.ds(0, DA)
    mine_r = pl.ds(pl.multiple_of(DR + QR * t, 128), QR)
    rest_r = pl.ds(0, DR)
    for c in tp_copies(
        4, lambda j: ffn_own.at[:, :, pl.ds(pl.multiple_of(DA + QB * j, 128), QB)], g_quarter.at[t]
    ):
        c.start()
    for c in tp_copies(6, lambda j: ffn_own.at[:, :, rest], g_rest.at[t]):
        c.start()
    g_quarter[t] = ffn_own[:, :, mine]
    g_rest[t] = ffn_own[:, :, rest]
    for c in (c_wg, c_wu, c_wd):
        c.wait()
    with jax.named_scope("wait_tp4"):
        tp_wait(4, g_quarter.at[0:3], g_quarter.at[0:3])
    def ep_send(src, dst, ssem, rsem, shift):
        pltpu.make_async_remote_copy(
            src_ref=src,
            dst_ref=dst,
            send_sem=ssem,
            recv_sem=rsem,
            device_id={"ep": shift},
            device_id_type=MESH,
        ).start()

    X[:, :, mine] = (
        mm(Dm[...], g_quarter[...].reshape(TP * PAD, QB)).astype(bf16).reshape(EP, CAPP, QB)
    )
    for p in range(EP - 1):
        to = ep_shift(me, order[p], 1)
        ep_send(X.at[p, :, mine], R.at[p, :, mine], dsb, drb.at[p // CHUNK], to)
    R[EP - 1, :, mine] = X[EP - 1, :, mine]
    with jax.named_scope("wait_tp6"):
        tp_wait(6, g_rest.at[0:3], g_rest.at[0:3])
    rows_rest = g_rest[...].reshape(TP * PAD, DA)
    for k in range(4):
        n = EP // 4
        X[k * n : (k + 1) * n, :, rest] = (
            mm(Dm[k * n * CAPP : (k + 1) * n * CAPP, :], rows_rest)
            .astype(bf16)
            .reshape(n, CAPP, DA)
        )
        for p in range(k * n, min((k + 1) * n, EP - 1)):
            to = ep_shift(me, order[p], 1)
            ep_send(X.at[p, :, rest], R.at[p, :, rest], dss, drs.at[p // CHUNK], to)
    R[EP - 1, :, rest] = X[EP - 1, :, rest]
    chunks = [(k, k * CHUNK, (k + 1) * CHUNK, min((k + 1) * CHUNK, EP - 1)) for k in range(EP // CHUNK)]
    for k, lo, hi, last in chunks:
        with jax.named_scope(f"wait_quarter{k}"):
            arrived(R.at[lo:last, :, mine], drb.at[k])
        for d in (2, 1, 3):
            pltpu.make_async_remote_copy(
                src_ref=R.at[lo:hi, :, mine],
                dst_ref=R.at[lo:hi, :, mine],
                send_sem=xgs.at[k],
                recv_sem=xgr.at[k],
                device_id={"tp": (t + d) % TP},
                device_id_type=MESH,
            ).start()

    def sum_chunk(k, lo, hi, last):
        with jax.named_scope(f"wait_sum{k}"):
            arrived(YB.at[0:3, lo:hi], ybr.at[k])
        summed = YB[0, lo:hi].astype(f32)
        for j in range(1, TP):
            summed = summed + YB[j, lo:hi].astype(f32)
        SB[lo:hi] = summed.astype(bf16)
        for p in range(lo, last):
            to = ep_shift(me, order[p], -1)
            ep_send(SB.at[p], T.at[p, :, mine_r], sbs, sbr, to)

    for k, lo, hi, last in chunks:
        with jax.named_scope(f"wait_dispatch{k}"):
            arrived(R.at[lo:last, :, rest], drs.at[k])
        with jax.named_scope(f"wait_gather{k}"):
            arrived(R.at[lo:hi, :, 0 : 3 * QB], xgr.at[k])
        flat = R[lo:hi].reshape(CHUNK * CAPP, D)
        gate = jnp.minimum(mm(flat, wg[...]), clamp_limit)
        upward = jnp.clip(mm(flat, wu[...]), -clamp_limit, clamp_limit)
        active = ((upward + 1.0) * gate * jax.nn.sigmoid(sigmoid_alpha * gate)).astype(bf16)
        Y[lo:hi] = mm(active, wd[...]).astype(bf16).reshape(CHUNK, CAPP, D)
        for d in (2, 1, 3):
            j = (t + d) % TP
            pltpu.make_async_remote_copy(
                src_ref=Y.at[lo:hi, :, pl.ds(pl.multiple_of(DR + QR * j, 128), QR)],
                dst_ref=YB.at[t, lo:hi],
                send_sem=ybs.at[k],
                recv_sem=ybr.at[k],
                device_id={"tp": j},
                device_id_type=MESH,
            ).start()
        for p in range(lo, last):
            to = ep_shift(me, order[p], -1)
            ep_send(Y.at[p, :, rest_r], T.at[p, :, rest_r], ess, ers, to)
        YB[t, lo:hi] = Y[lo:hi, :, mine_r]
        if k >= LAG:
            sum_chunk(*chunks[k - LAG])
    T[EP - 1, :, rest_r] = Y[EP - 1, :, rest_r]
    for k in range(max(0, len(chunks) - LAG), len(chunks)):
        sum_chunk(*chunks[k])
    T[EP - 1, :, mine_r] = SB[EP - 1]
    with jax.named_scope("wait_return"):
        arrived(T.at[0 : EP - 1, :, rest_r], ers)
    with jax.named_scope("wait_return_sum"):
        arrived(SB.at[0 : EP - 1], sbr)
    for at, wide, cols in ((0, DR, rest_r), (DR, QR, mine_r)):
        both = mm(Cm[...], T[:, :, cols].reshape(EP * CAPP, wide))
        m_s[:, :, :, at : at + wide] = (
            (both[0 : TP * PAD] + both[TP * PAD :]).astype(bf16).reshape(TP, 3, 4, wide)
        )
    ph5 = tp_copies(5, lambda j: m_s.at[j], m_r.at[t])
    for c in ph5:
        c.start()
    m_r[t] = m_s[t]
    with jax.named_scope("wait_tp5"):
        tp_wait(5, m_s.at[0:3], m_r.at[0:3])
    arrived(X.at[0 : EP - 1, :, rest], dss)
    arrived(X.at[0 : EP - 1, :, mine], dsb)
    arrived(Y.at[0 : EP - 1, :, rest_r], ess)
    arrived(SB.at[0 : EP - 1], sbs)
    for k, lo, hi, last in chunks:
        arrived(R.at[lo:hi, :, 0 : 3 * QB], xgs.at[k])
        arrived(YB.at[0:3, lo:hi], ybs.at[k])
    with jax.named_scope("final"):
      moe = m_r[0, :, :, 0:DR].reshape(PAD, DR).astype(f32)
      for j in range(1, TP):
        moe = moe + m_r[j, :, :, 0:DR].reshape(PAD, DR).astype(f32)
      parts = [m_r[j, :, :, DR:].reshape(PAD, QR).astype(f32) for j in range(TP)]
      moe = jnp.concatenate([moe] + parts, axis=1)
      moe = moe.astype(bf16).astype(f32)
      res = (mixed_ref[...] + rms(moe, g_post2[...].astype(f32))).astype(bf16)
      out_ref[...] = res


def finish_kernel(a, b, c, x, y, z, sem):
    copies = [pltpu.make_async_copy(p, q, sem.at[i]) for i, (p, q) in enumerate(((a, x), (b, y), (c, z)))]
    for p in copies:
        p.start()
    for p in copies:
        p.wait()


def body(
    tokens,
    cache_latent,
    cache_rope,
    lengths,
    attn_gain,
    latent_gain,
    post_attn_gain,
    ffn_gain,
    post_ffn_gain,
    w_query,
    w_query_rot,
    w_latent,
    w_key_rot,
    w_key_up,
    w_value_up,
    w_out,
    route_logits,
    routes,
    w_gate,
    w_up,
    w_down,
):
    vm = pl.BlockSpec(memory_space=pltpu.VMEM)
    hbm = pl.BlockSpec(memory_space=pl.ANY)
    V = pltpu.VMEM
    scratch = [
        pltpu.SMEM((SEQ,), jnp.int32),
        V((SEQ, D), bf16),
        V((4, TP * SEQ), jnp.int32),
        V((4, TP * SEQ), f32),
        V((D,), bf16),
        V((LAT,), bf16),
        V((D,), bf16),
        V((D,), bf16),
        V((D,), bf16),
        V((PAD, D), f32),
        V((TP, 3, 4, D), bf16),
        V((D, 512), bf16),
        V((D, 256), bf16),
        V((D, 128), bf16),
        V((ROT, D), bf16),
        V((HL * LAT, 128), bf16),
        V((HL * LAT, 128), bf16),
        V((2, HL * LAT, 128), f32),
        V((HL, LAT, 128), bf16),
        V((HL, LAT, 128), bf16),
        V((TP, 3, 4, MSG), bf16),
        V((TP, 3, 4, MSG), bf16),
        V((SEQ, LEN, LAT), bf16),
        V((SEQ, LAT, LEN), bf16),
        V((SEQ, ROT, LEN), bf16),
        V((LAT // 128, 16 * PAD, 128), f32),
        V((16 * PAD, 128), f32),
        V((SEQ, 16, LAT), bf16),
        V((SEQ, 16, 128), bf16),
        V((SEQ, 16, LEN), f32),
        V((SEQ, 16, LEN), bf16),
        V((SEQ, 16, 128), f32),
        V((LAT // 128, 16 * PAD, 128), f32),
        V((3, TP, HL, 4, LAT), bf16),
        V((3, TP, HL, 4, LAT), bf16),
        V((512, D), bf16),
        V((3, TP, 4, D), bf16),
        V((TP, 3, 4, D), bf16),
        V((3, 4, D), bf16),
        V((TP, 3, 4, QB), bf16),
        V((TP, 3, 4, DA), bf16),
        V((PAD, D), f32),
        V((EP * CAPP, TP * PAD), bf16),
        V((2 * TP * PAD, EP * CAPP), bf16),
        V((EP, CAPP, D), bf16),
        V((EP, CAPP, D), bf16),
        V((EP, CAPP, D), bf16),
        V((EP, CAPP, D), bf16),
        V((D, 512), bf16),
        V((D, 512), bf16),
        V((512, D), bf16),
        V((TP, 3, 4, DR + QR), bf16),
        V((TP, 3, 4, DR + QR), bf16),
        pltpu.SemaphoreType.DMA((19,)),
        pltpu.SemaphoreType.DMA((SEQ,)),
        pltpu.SemaphoreType.DMA,
        pltpu.SemaphoreType.DMA((7,)),
        pltpu.SemaphoreType.DMA((7,)),
        pltpu.SemaphoreType.DMA,
        pltpu.SemaphoreType.DMA,
        V((TP, EP, CAPP, QR), bf16),
        V((EP, CAPP, QR), bf16),
        pltpu.SemaphoreType.DMA,
        pltpu.SemaphoreType.DMA((EP // CHUNK,)),
        pltpu.SemaphoreType.DMA,
        pltpu.SemaphoreType.DMA,
        pltpu.SemaphoreType.DMA,
        pltpu.SemaphoreType.DMA((EP // CHUNK,)),
        pltpu.SemaphoreType.DMA((EP // CHUNK,)),
        pltpu.SemaphoreType.DMA((EP // CHUNK,)),
        pltpu.SemaphoreType.DMA((EP // CHUNK,)),
        pltpu.SemaphoreType.DMA((EP // CHUNK,)),
        pltpu.SemaphoreType.DMA,
        pltpu.SemaphoreType.DMA,
    ]
    parts = pl.pallas_call(
        layer_kernel,
        name="layer",
        out_shape=(
            pltpu.VMEM((SEQ, D), bf16),
            pltpu.VMEM((SEQ, LAT), bf16),
            pltpu.VMEM((SEQ, ROT), bf16),
        ),
        in_specs=[hbm] * 21,
        out_specs=(vm, vm, vm),
        scratch_shapes=scratch,
        compiler_params=pltpu.CompilerParams(
            collective_id=0, has_side_effects=True, vmem_limit_bytes=60 * 1024 * 1024
        ),
    )(
        lengths,
        tokens,
        routes.T,
        route_logits.T,
        attn_gain,
        latent_gain,
        post_attn_gain,
        ffn_gain,
        post_ffn_gain,
        cache_latent,
        cache_rope,
        w_query,
        w_query_rot,
        w_latent,
        w_key_rot.T,
        w_key_up.reshape(-1, w_key_up.shape[2]),
        w_value_up.reshape(-1, w_value_up.shape[2]),
        w_out,
        w_gate,
        w_up,
        w_down,
    )
    parts = [pltpu.with_memory_space_constraint(p, pltpu.VMEM) for p in parts]
    return pl.pallas_call(
        finish_kernel,
        name="finish",
        out_shape=(
            jax.ShapeDtypeStruct((SEQ, D), bf16),
            jax.ShapeDtypeStruct((SEQ, LAT), bf16),
            jax.ShapeDtypeStruct((SEQ, ROT), bf16),
        ),
        in_specs=[vm] * 3,
        out_specs=(hbm,) * 3,
        scratch_shapes=[pltpu.SemaphoreType.DMA((3,))],
    )(*parts)


def solution(mesh):
    return jax.shard_map(
        body,
        mesh=mesh,
        in_specs=(
            P(("ep", "tp"), None),
            P(("ep", "tp"), None, None),
            P(("ep", "tp"), None, None),
            P(("ep", "tp")),
            P(),
            P(),
            P(),
            P(),
            P(),
            P(None, "tp"),
            P(None, "tp"),
            P(None, "tp"),
            P(),
            P(None, "tp", None),
            P(None, "tp", None),
            P("tp", None),
            P("ep", None),
            P("ep", None),
            P("ep", None, "tp"),
            P("ep", None, "tp"),
            P("ep", "tp", None),
        ),
        out_specs=(P(("ep", "tp"), None), P(("ep", "tp"), None), P(("ep", "tp"), None)),
        check_vma=False,
    )
```
